128 devices in a mesh: ep: 64 (over z, y, x), tp: 2 (over core).
Axes of the slice: x: 4, y: 4, z: 4, core: 2. Of those that a mesh axis runs over, the one named last changes fastest.
Arguments:
- residual: bfloat16 [4096, 2048], P('ep', 'tp'), may hold values from -100 to 100
- route_ids: int32 [4096, 4], P('ep'), may hold values from 0 to 63, all different within a row; in each aligned block of 64 rows (0 to 63, 64 to 127, ...) at most 6 rows name the same one
- route_weights: float32 [4096, 4], P('ep'), may hold values from 0.1 to 1
- carried_state: float32 [2, 4096, 4096], P(None, 'ep', 'tp'), may hold values from -6 to 6
- mix_gain: float32 [2048], replicated, may hold values from 0.1 to 1.9
- in_proj: bfloat16 [2048, 1024], P(None, 'tp'), may hold values from -0.125 to 0.125
- decay_rate: float32 [64, 64], P('tp'), may hold values from 0.1 to 2
- frequency: float32 [64, 64], P('tp'), may hold values from -3 to 3
- step_size: float32 [64], P('tp'), may hold values from 0.05 to 1
- input_map: float32 [2, 64, 64, 16], P(None, 'tp'), may hold values from -1.5 to 1.5
- output_matrix: float32 [2, 64, 16, 64], P(None, 'tp'), may hold values from -0.5 to 0.5
- passthrough_scale: float32 [1024], P('tp'), may hold values from -4 to 4
- out_gain: float32 [1024], replicated, may hold values from 0.1 to 1.9
- out_proj: bfloat16 [1024, 2048], P(None, 'tp'), may hold values from -0.1875 to 0.1875
- ffn_gain: float32 [2048], replicated, may hold values from 0.1 to 1.9
- w_gate: bfloat16 [64, 2048, 2048], P('ep', None, 'tp'), may hold values from -5 to 5
- w_up: bfloat16 [64, 2048, 2048], P('ep', None, 'tp'), may hold values from -5 to 5
- w_down: bfloat16 [64, 2048, 2048], P('ep', 'tp'), may hold values from -0.125 to 0.125
Outputs:
- updated: bfloat16 [4096, 2048], P('ep', 'tp')
- new_state: float32 [2, 4096, 4096], P(None, 'ep', 'tp')
The draws below stay inside these ranges and needn't reach their ends.
Inputs may be any that keep to these rules, and one draw needn't show every extreme that they name: `route_ids`: each row names 4 different experts. Among the 64 rows of one device (aligned blocks) no expert is named more than 6 times, and in every draw some block names some expert exactly 6 times.
All inputs are finite; a program needn't handle non-finite values.
Results may differ from the reference program's by a relative error of at most 0.018.
Values may be sent and summed in bfloat16 or wider, within the bound.
A program may use at most 128 MiB of HBM per device.

```python
import math
import jax
import jax.numpy as jnp
import numpy as np
from jax import lax

D = 2048
S5W = 1024
GROUP_CH = 16
GROUPS = 64
STATE = 64
FF = 2048
EXPERTS = 64
TOPK = 4
SEQ_DEV = 64
TOKENS = 4096
CAP = 6
WIDTH_SPLIT = 2
N_EP = 64


def draw_residual(key, part):
    key_one = jax.random.fold_in(key, 11)
    key_three = jax.random.fold_in(key, 13)
    column_pos = jnp.arange(D, dtype=jnp.float32) / D
    column_ramp = jnp.exp(math.log(3.0) * column_pos)
    base_draw = jnp.clip(jax.random.normal(key_one, (TOKENS, D), jnp.float32), -5.0, 5.0)
    jitter = jnp.exp(jax.random.uniform(key_three, (1, D), jnp.float32, -0.35, 0.35))
    return (base_draw * column_ramp * jitter / 1.5).astype(jnp.bfloat16)


def expert_weight(key, salt_value):
    key_one = jax.random.fold_in(key, salt_value)
    key_two = jax.random.fold_in(key, salt_value + 1)
    base_draw = jnp.clip(jax.random.normal(key_one, (EXPERTS, D, FF), jnp.float32), -5.0, 5.0) / math.sqrt(D)
    top_scale = 3.0
    column_scale = 0.5 * jnp.exp(jax.random.uniform(key_two, (EXPERTS, 1, FF), jnp.float32, 0.0, math.log(top_scale / 0.5)))
    return (base_draw * column_scale).astype(jnp.bfloat16)


def draw_w_gate(key, part):
    return expert_weight(key, 21)


def draw_w_up(key, part):
    return expert_weight(key, 31)


def block_levels(stream_key, dims, split, smallest, largest):
    factor_of = 1.0
    for axis_at, shards_of in split:
        heights = jax.random.uniform(jax.random.fold_in(jax.random.fold_in(stream_key, 6), axis_at), (shards_of,), jnp.float32, smallest / len(split), largest / len(split))
        factor_of = factor_of * jnp.repeat(jnp.exp(heights), dims[axis_at] // shards_of).reshape((-1,) + (1,) * (len(dims) - 1 - axis_at))
    return factor_of


def deal_out(own_key, own, number, rows, count, top, limit, lean):
    ranking = jax.random.permutation(own_key, count)
    packed, common = load_shares(count, rows * top, limit, lean, True), load_shares(count, rows * top, limit, lean, False)
    places = jnp.arange(count)

    def named(tallies, turn):
        used = int((tallies > 0).sum())
        fixed = max(1, used // 4)
        moved = fixed + (places - fixed + turn * (used - fixed)) % max(1, count - fixed)
        return jnp.zeros((count,), jnp.int32).at[ranking[jnp.where(places < fixed, places, moved)]].set(jnp.asarray(tallies, jnp.int32))

    tallies = jnp.where(number % 4 == 0, named(packed, number // 4), named(common, number - number // 4 - 1))
    mixed = jax.random.permutation(jax.random.fold_in(own, 3), count)
    source_of, taker = mixed[0:count // 2 * 2:2], mixed[1:count // 2 * 2:2]
    slack = jnp.minimum(tallies[source_of] - 1, limit - tallies[taker]) // 2
    slack = jnp.where((source_of == ranking[0]) | (taker == ranking[0]) | (tallies[taker] == 0), 0, jnp.maximum(slack, 0))
    moved = jax.random.randint(jax.random.fold_in(own, 4), (count // 2,), 0, 1 << 20) % (slack + 1)
    tallies = tallies.at[source_of].add(-moved).at[taker].add(moved)
    labels = jnp.searchsorted(jnp.cumsum(tallies), jnp.arange(rows * top), side="right").astype(jnp.int32)
    grid = labels.reshape(top, rows).T
    grid = grid[jax.random.permutation(jax.random.fold_in(own, 1), rows)]
    turn = jax.random.randint(jax.random.fold_in(own, 2), (rows, 1), 0, top)
    return jnp.take_along_axis(grid, (jnp.arange(top)[None, :] + turn) % top, axis=1)


def load_shares(count, total, bound, slope, full):
    portions = [(1 << 20) // math.isqrt(grade ** slope) + 1 for grade in range(1, count + 1)]
    largest = bound if full else min(bound, max(-(-total // count), total * portions[0] // sum(portions)))
    least = 1 if total - largest >= count - 1 else 0
    counts, surplus = [largest] + [least] * (count - 1), total - largest - least * (count - 1)
    while surplus > 0:
        free = [i for i in range(1, count) if counts[i] < largest] or [i for i in range(1, count) if counts[i] < bound]
        pool, left = sum([portions[i] for i in free]), surplus
        for i in free:
            addition = min(bound - counts[i], max(1, left * portions[i] // pool), surplus)
            counts[i] = counts[i] + addition
            surplus = surplus - addition
    return np.array(counts)


def scatter_about(own_key, shape, scale, bound, cuts=(), kind=jnp.bfloat16):
    factor_of = block_levels(own_key, shape, cuts, -0.22, 0.18) if cuts else 1.0
    entries = jax.random.normal(own_key, shape, jnp.float32) * scale * factor_of
    return jnp.minimum(jnp.maximum(entries, -bound), bound).astype(kind)


def setup_inputs(seed: int = 0) -> dict:
    arg_keys = jax.random.split(jax.random.key(seed), 19)
    residual = draw_residual(jax.random.fold_in(arg_keys[18], 71), 0)
    route_ids_keys = jax.random.split(jax.random.fold_in(arg_keys[1], 1), TOKENS // SEQ_DEV)
    route_ids_turns = jax.random.permutation(jax.random.fold_in(arg_keys[1], 3), TOKENS // SEQ_DEV)
    route_ids = jax.vmap(lambda own, number: deal_out(jax.random.fold_in(arg_keys[1], 2), own, number, SEQ_DEV, EXPERTS, TOPK, CAP, 1))(route_ids_keys, route_ids_turns).reshape((TOKENS, TOPK))
    route_weights = jnp.clip(0.1 + 0.9 * jax.random.uniform(arg_keys[2], (TOKENS, TOPK), jnp.float32) ** block_levels(arg_keys[2], (TOKENS, TOPK), ((0, 64),), -0.2, 0.2), 0.1, 1.0)
    carried_state = scatter_about(arg_keys[3], (2, TOKENS, GROUPS * STATE), 1.0, 6.0, ((1, 64), (2, 2)), jnp.float32)
    mix_gain = jnp.clip(1.0 + 0.18 * jax.random.normal(arg_keys[4], (D,), jnp.float32), 0.1, 1.9)
    in_proj = scatter_about(arg_keys[5], (D, S5W), D ** -0.5, 0.125, ((1, 2),))
    decay_rate = jnp.clip(jnp.exp(math.log(2.0) - 2.9957323 * jax.random.uniform(arg_keys[6], (GROUPS, STATE), jnp.float32) ** block_levels(arg_keys[6], (GROUPS, STATE), ((0, 2),), -0.2, 0.2)), 0.1, 2.0)
    frequency = jnp.clip(jax.random.uniform(arg_keys[7], (GROUPS, STATE), jnp.float32, -3.0, 3.0) * block_levels(arg_keys[7], (GROUPS, STATE), ((0, 2),), -0.4, 0.0), -3.0, 3.0)
    step_size = jnp.clip(jnp.exp(math.log(1.0) - 2.9957323 * jax.random.uniform(arg_keys[8], (GROUPS,), jnp.float32) ** block_levels(arg_keys[8], (GROUPS,), ((0, 2),), -0.2, 0.2)), 0.05, 1.0)
    input_map = scatter_about(arg_keys[9], (2, GROUPS, STATE, GROUP_CH), GROUP_CH ** -0.5, 1.5, ((1, 2),), jnp.float32)
    output_matrix = scatter_about(arg_keys[10], (2, GROUPS, GROUP_CH, STATE), (2 * STATE) ** -0.5, 0.5, ((1, 2),), jnp.float32)
    passthrough_scale = scatter_about(arg_keys[11], (S5W,), 1.0, 4.0, ((0, 2),), jnp.float32)
    out_gain = jnp.clip(1.0 + 0.18 * jax.random.normal(arg_keys[12], (S5W,), jnp.float32), 0.1, 1.9)
    out_proj = scatter_about(arg_keys[13], (S5W, D), S5W ** -0.5, 0.1875, ((1, 2),))
    ffn_gain = jnp.clip(1.0 + 0.18 * jax.random.normal(arg_keys[14], (D,), jnp.float32), 0.1, 1.9)
    w_gate = draw_w_gate(jax.random.fold_in(arg_keys[18], 71), 0)
    w_up = draw_w_up(jax.random.fold_in(arg_keys[18], 71), 0)
    w_down = scatter_about(arg_keys[17], (EXPERTS, FF, D), FF ** -0.5, 0.125, ((0, 64), (1, 2)))
    return {"residual": residual, "route_ids": route_ids, "route_weights": route_weights, "carried_state": carried_state, "mix_gain": mix_gain, "in_proj": in_proj, "decay_rate": decay_rate, "frequency": frequency, "step_size": step_size, "input_map": input_map, "output_matrix": output_matrix, "passthrough_scale": passthrough_scale, "out_gain": out_gain, "out_proj": out_proj, "ffn_gain": ffn_gain, "w_gate": w_gate, "w_up": w_up, "w_down": w_down}


epsilon = 1e-06
clamp_limit = 7.0
swish_alpha = 1.702

def rms_rows(values, gain_vec):
    return values * lax.rsqrt(lax.optimization_barrier(jnp.mean(values * values, axis=1, keepdims=True)) + epsilon) * gain_vec

def discretize(decay_rate, frequency, step_size):
    rate_real = -decay_rate
    rate_imag = frequency
    time_step = step_size[:, None]
    magnitude = jnp.exp(rate_real * time_step)
    phase_angle = rate_imag * time_step
    bar_real = magnitude * jnp.cos(phase_angle)
    bar_imag = magnitude * jnp.sin(phase_angle)
    denominator = rate_real * rate_real + rate_imag * rate_imag
    shifted = bar_real - 1.0
    coef_real = (shifted * rate_real + bar_imag * rate_imag) / denominator
    coef_imag = (bar_imag * rate_real - shifted * rate_imag) / denominator
    return (bar_real, bar_imag, coef_real, coef_imag)

def state_step(channels, carried_state, decay_rate, frequency, step_size, input_map, output_matrix, passthrough_scale):
    row_count = channels.shape[0]
    number_of_groups, state_width = decay_rate.shape
    channels_per_group = input_map.shape[3]
    bar_real, bar_imag, coef_real, coef_imag = discretize(decay_rate, frequency, step_size)
    map_real = coef_real[..., None] * input_map[0] - coef_imag[..., None] * input_map[1]
    map_imag = coef_real[..., None] * input_map[1] + coef_imag[..., None] * input_map[0]
    input_rows = channels.astype(jnp.float32).reshape(row_count, number_of_groups, channels_per_group)
    largest_precision = lax.Precision.HIGHEST
    push_real = jnp.einsum('sgc,gpc->sgp', input_rows, map_real, precision=largest_precision)
    push_imag = jnp.einsum('sgc,gpc->sgp', input_rows, map_imag, precision=largest_precision)
    old_real = carried_state[0].reshape(row_count, number_of_groups, state_width)
    old_imag = carried_state[1].reshape(row_count, number_of_groups, state_width)
    updated_real = bar_real * old_real - bar_imag * old_imag + push_real
    updated_imaginary = bar_real * old_imag + bar_imag * old_real + push_imag
    mixer_output = jnp.einsum('dfk,idk->idf', output_matrix[0], updated_real, precision=largest_precision) - jnp.einsum('dfk,idk->idf', output_matrix[1], updated_imaginary, precision=largest_precision) + passthrough_scale.reshape(number_of_groups, channels_per_group) * input_rows
    activated = jax.nn.gelu(mixer_output.reshape(row_count, number_of_groups * channels_per_group)).astype(jnp.bfloat16)
    new_state = jnp.stack([updated_real.reshape(row_count, -1), updated_imaginary.reshape(row_count, -1)])
    return (activated, new_state)

def expert_apply(expert_item):
    rows_in, gate_w, up_w, down_w = expert_item
    slot_count = rows_in.shape[0]
    gate_pre = jnp.dot(rows_in, gate_w, preferred_element_type=jnp.float32)
    up_pre = jnp.dot(rows_in, up_w, preferred_element_type=jnp.float32)
    gated = jnp.minimum(gate_pre, clamp_limit)
    activation = ((jnp.clip(up_pre, -clamp_limit, clamp_limit) + 1.0) * gated * jax.nn.sigmoid(swish_alpha * gated)).astype(jnp.bfloat16)
    block_width = FF // WIDTH_SPLIT
    pieces = jnp.einsum('mtf,tfd->mtd', activation.reshape(slot_count, WIDTH_SPLIT, block_width).astype(jnp.float32), down_w.reshape(WIDTH_SPLIT, block_width, D).astype(jnp.float32))
    pieces = lax.optimization_barrier(pieces.astype(jnp.bfloat16)).astype(jnp.float32)
    return lax.optimization_barrier(jnp.sum(pieces, axis=1)).astype(jnp.bfloat16)

def reference(residual, route_ids, route_weights, carried_state, mix_gain, in_proj, decay_rate, frequency, step_size, input_map, output_matrix, passthrough_scale, out_gain, out_proj, ffn_gain, w_gate, w_up, w_down):
    start_rows = residual.astype(jnp.float32)
    normed_rows = rms_rows(start_rows, mix_gain).astype(jnp.bfloat16)
    channels = jnp.dot(normed_rows, in_proj, preferred_element_type=jnp.float32).astype(jnp.bfloat16)
    activated, new_state = state_step(channels, carried_state, decay_rate, frequency, step_size, input_map, output_matrix, passthrough_scale)
    scaled = rms_rows(activated.astype(jnp.float32), out_gain).astype(jnp.bfloat16)
    after_mixer = (start_rows + jnp.dot(scaled, out_proj, preferred_element_type=jnp.float32)).astype(jnp.bfloat16)
    expert_in = rms_rows(after_mixer.astype(jnp.float32), ffn_gain).astype(jnp.bfloat16)
    route_count = TOKENS * TOPK
    flat_ids = route_ids.reshape(route_count).astype(jnp.int32)
    onehot = (flat_ids[:, None] == jnp.arange(EXPERTS, dtype=jnp.int32)[None, :]).astype(jnp.int32)
    blocked = onehot.reshape(N_EP, SEQ_DEV * TOPK, EXPERTS)
    before = (jnp.cumsum(blocked, axis=1).astype(jnp.int32) - blocked).reshape(route_count, EXPERTS)
    slot_index = lax.optimization_barrier(jnp.sum(before * onehot, axis=1)).astype(jnp.int32)
    route_iota = jnp.arange(route_count, dtype=jnp.int32)
    block_index = (route_iota // (SEQ_DEV * TOPK)).astype(jnp.int32)
    slot_total = N_EP * CAP
    position = (flat_ids * slot_total + block_index * CAP + slot_index).astype(jnp.int32)
    source_row = (route_iota // TOPK).astype(jnp.int32)
    row_table = jnp.full((EXPERTS * slot_total,), TOKENS, dtype=jnp.int32).at[position].set(source_row)
    padded = jnp.concatenate([expert_in, jnp.zeros((1, D), jnp.bfloat16)], axis=0)
    gathered = padded[row_table].reshape(EXPERTS, slot_total, D)
    outputs = lax.map(expert_apply, (gathered, w_gate, w_up, w_down))
    picked = outputs.reshape(EXPERTS * slot_total, D)[position].reshape(TOKENS, TOPK, D)
    expert_sum = lax.optimization_barrier(jnp.sum(route_weights[:, :, None] * picked.astype(jnp.float32), axis=1))
    updated = (after_mixer.astype(jnp.float32) + expert_sum).astype(jnp.bfloat16)
    return (updated, new_state)
```

```python
import jax
import jax.numpy as jnp
from jax import lax
from jax.experimental import pallas as pl
from jax.experimental.pallas import tpu as pltpu
from jax.sharding import PartitionSpec as P

F32 = jnp.float32
BF16 = jnp.bfloat16
MESH = pl.DeviceIdType.MESH

EPS = 1e-06
LIMIT = 7.0
ALPHA = 1.702

SEQ = 64
HALF = 1024
STATES = 2048
CHAN = 512
PEERS = 64
SLOTS = 6
QUARTERS = 4
QW = HALF // QUARTERS
ROWS = SLOTS * QUARTERS
ALL = PEERS * ROWS
PAD = ALL + 8
GROUPS = 4
GP = PEERS // GROUPS
GROWS = GP * ROWS
GSLOTS = GP * SLOTS
BLK = 8 * ROWS
BSLOTS = 8 * SLOTS
ZSTEP = (0, 1, 3, 2)
CHUNKS = ((0, 1), (2, 3))

NT = (((1,), (1,)), ((), ()))


def mm(a, b):
    return jnp.dot(a, b, preferred_element_type=F32)


def mm_nt(a, b):
    return lax.dot_general(a, b, NT, preferred_element_type=F32)


def iota(shape, dim):
    return lax.broadcasted_iota(jnp.int32, shape, dim)


def div_small(v, d):
    return ((v.astype(F32) + 0.5) * (1.0 / d)).astype(jnp.int32)


def kernel(
    xg,
    ids_in,
    wts_in,
    state_in,
    mix_gain_in,
    in_proj_in,
    decay_in,
    freq_in,
    step_in,
    imap_in,
    omap_in,
    pscale_in,
    out_gain_in,
    out_proj_in,
    ffn_gain_in,
    wg_in,
    wu_in,
    wd_in,
    out_ref,
    nstate_ref,
    xv,
    ids,
    wts,
    state,
    mix_gain,
    in_proj,
    decay,
    freq,
    step,
    imap,
    omap,
    pscale,
    out_gain,
    out_proj,
    ffn_gain,
    wg,
    wu,
    wd,
    outv,
    nstate,
    actx,
    sqx,
    onehot,
    chi,
    clo,
    perm,
    permt,
    sendbuf,
    recv,
    rsend,
    rrecv,
    amat,
    hid,
    psend,
    prec,
    in_sems,
    out_sems,
    x_send,
    x_recv,
    d_send,
    d_recv,
    f_send,
    f_recv,
    p_send,
    p_recv,
    r_send,
    r_recv,
):
    ep = lax.axis_index("ep")
    tp = lax.axis_index("tp")
    other = 1 - tp
    z = lax.div(ep, 16)
    y = lax.rem(lax.div(ep, 4), 4)
    x = lax.rem(ep, 4)

    def peer_of(zstep, j, sign):
        dy = lax.div(j, 4)
        dx = lax.rem(j, 4)
        pz = lax.rem(z + sign * zstep + 4, 4)
        py = lax.rem(y + sign * dy + 4, 4)
        px = lax.rem(x + sign * dx + 4, 4)
        return pz * 16 + py * 4 + px

    barrier = pltpu.get_barrier_semaphore()
    pl.semaphore_signal(barrier, inc=1, device_id=(ep, other), device_id_type=MESH)
    for g in range(GROUPS):

        def greet(j, carry, g=g):
            pl.semaphore_signal(
                barrier, inc=1, device_id=(peer_of(ZSTEP[g], j, 1), tp), device_id_type=MESH
            )
            return carry

        lax.fori_loop(1 if g == 0 else 0, GP, greet, 0)

    pairs = (
        (xg, xv),
        (ids_in, ids),
        (wts_in, wts),
        (mix_gain_in, mix_gain),
        (in_proj_in, in_proj),
        (decay_in, decay),
        (freq_in, freq),
        (step_in, step),
        (imap_in, imap),
        (state_in, state),
        (omap_in, omap),
        (pscale_in, pscale),
        (out_gain_in, out_gain),
        (out_proj_in, out_proj),
        (ffn_gain_in, ffn_gain),
        (wg_in, wg),
        (wu_in, wu),
        (wd_in, wd),
    )
    loads = [pltpu.make_async_copy(a, b, in_sems.at[i]) for i, (a, b) in enumerate(pairs)]
    for load in loads:
        load.start()

    loads[1].wait()
    loads[2].wait()
    expert = iota((PEERS, SEQ), 0)
    named = jnp.zeros((PEERS, SEQ), F32)
    weight = jnp.zeros((PEERS, SEQ), F32)
    for k in range(4):
        hit = ids[k : k + 1, :] == expert
        named = named + jnp.where(hit, 1.0, 0.0)
        weight = weight + jnp.where(hit, wts[k : k + 1, :], 0.0)
    earlier = jnp.where(iota((SEQ, SEQ), 0) < iota((SEQ, SEQ), 1), 1.0, 0.0).astype(BF16)
    slot_of = named * (mm(named.astype(BF16), earlier) + 1.0)
    pos = iota((PEERS, PEERS), 0)
    gz = pos >> 4
    pz = (z + (gz ^ (gz >> 1))) & 3
    py = (y + ((pos >> 2) & 3)) & 3
    px = (x + (pos & 3)) & 3
    order = jnp.where(pz * 16 + py * 4 + px == iota((PEERS, PEERS), 1), 1.0, 0.0).astype(BF16)
    w_hi = weight.astype(BF16)
    w_lo = (weight - w_hi.astype(F32)).astype(BF16)
    slot_pt = mm(order, slot_of.astype(BF16)).astype(BF16)
    eye = jnp.where(iota((SEQ, SEQ), 0) == iota((SEQ, SEQ), 1), 1.0, 0.0).astype(BF16)

    def turned(v):
        return mm_nt(eye, v).astype(BF16)

    slot_tp = turned(slot_pt)
    whi_tp = turned(mm(order, w_hi).astype(BF16))
    wlo_tp = turned(mm(order, w_lo).astype(BF16))

    slot_p4 = jnp.concatenate([slot_pt] * QUARTERS, axis=1)
    row = iota((BLK, QUARTERS * SEQ), 0)
    rowp = div_small(row, ROWS)
    rem_row = row - rowp * ROWS
    rowq = div_small(rem_row, SLOTS)
    rows_ = rem_row - rowq * SLOTS
    want = jnp.where(rowq == (iota((BLK, QUARTERS * SEQ), 1) >> 6), rows_ + 1, -1).astype(F32)
    spread_row = div_small(iota((BLK, PEERS), 0), ROWS)
    spread_col = iota((BLK, PEERS), 1)
    for b in range(PEERS // 8):
        spread = jnp.where(spread_row + b * 8 == spread_col, 1.0, 0.0).astype(BF16)
        onehot[b * BLK : (b + 1) * BLK, :] = jnp.where(
            mm(spread, slot_p4) == want, 1.0, 0.0
        ).astype(BF16)

    def block_perm(rdim, cdim):
        r = iota((BLK, BLK), rdim)
        c = iota((BLK, BLK), cdim)
        rq = div_small(r, BSLOTS)
        rr = r - rq * BSLOTS
        rp = div_small(rr, SLOTS)
        rs = rr - rp * SLOTS
        return jnp.where(rp * ROWS + rq * SLOTS + rs == c, 1.0, 0.0).astype(BF16)

    perm[...] = block_perm(0, 1)
    permt[...] = block_perm(1, 0)

    loads[5].wait()
    loads[6].wait()
    loads[7].wait()
    rate_real = -decay[...]
    rate_imag = freq[...]
    n_groups, n_state = rate_real.shape
    diag = iota((n_groups, n_groups), 0) == iota((n_groups, n_groups), 1)
    time_step = jnp.sum(jnp.where(diag, step[...], 0.0), axis=1, keepdims=True)
    magnitude = jnp.exp(rate_real * time_step)
    phase = rate_imag * time_step
    bar_real = magnitude * jnp.cos(phase)
    bar_imag = magnitude * jnp.sin(phase)
    denominator = rate_real * rate_real + rate_imag * rate_imag
    shifted = bar_real - 1.0
    coef_real = (shifted * rate_real + bar_imag * rate_imag) / denominator
    coef_imag = (bar_imag * rate_real - shifted * rate_imag) / denominator
    own_group = iota((n_groups, STATES), 0) == (iota((n_groups, STATES), 1) >> 6)

    def as_row(v):
        wide = jnp.concatenate([v] * (STATES // n_state), axis=1)
        return jnp.sum(jnp.where(own_group, wide, 0.0), axis=0, keepdims=True)

    bar_real, bar_imag, coef_real, coef_imag = (
        as_row(v) for v in (bar_real, bar_imag, coef_real, coef_imag)
    )

    loads[0].wait()
    loads[3].wait()
    x0 = xv[0].astype(F32)
    x1 = xv[1].astype(F32)
    mean_sq = (
        jnp.sum(x0 * x0, axis=1, keepdims=True) + jnp.sum(x1 * x1, axis=1, keepdims=True)
    ) * (1.0 / (2 * HALF))
    scale = lax.rsqrt(mean_sq + EPS)
    n0 = (x0 * scale * mix_gain[:, :HALF]).astype(BF16)
    n1 = (x1 * scale * mix_gain[:, HALF:]).astype(BF16)
    loads[4].wait()
    channels = (mm(n0, in_proj[:HALF, :]) + mm(n1, in_proj[HALF:, :])).astype(BF16)
    loads[8].wait()
    loads[9].wait()
    loads[10].wait()
    loads[11].wait()
    same = (iota((128, 512), 0) >> 4) == (iota((128, 512), 1) >> 6)

    def spread_groups(m):
        return jnp.where(same, jnp.concatenate([m] * 8, axis=1), 0.0).astype(BF16)

    for b in range(4):
        rows = slice(b * 128, (b + 1) * 128)
        cols = slice(b * 512, (b + 1) * 512)
        ch = channels[:, rows]
        u0 = mm(ch, spread_groups(imap[0, rows, :]))
        u1 = mm(ch, spread_groups(imap[1, rows, :]))
        hr = state[0, :, cols]
        hi = state[1, :, cols]
        br, bi = bar_real[:, cols], bar_imag[:, cols]
        cr, ci = coef_real[:, cols], coef_imag[:, cols]
        nr = br * hr - bi * hi + (cr * u0 - ci * u1)
        ni = br * hi + bi * hr + (cr * u1 + ci * u0)
        nstate[0, :, cols] = nr
        nstate[1, :, cols] = ni
        mixed = (
            mm_nt(nr.astype(BF16), spread_groups(omap[0, rows, :]))
            - mm_nt(ni.astype(BF16), spread_groups(omap[1, rows, :]))
            + pscale[:, rows] * ch.astype(F32)
        )
        actx[tp, :, rows] = jax.nn.gelu(mixed, approximate=True).astype(BF16)
    store_state = pltpu.make_async_copy(nstate, nstate_ref, out_sems.at[0])
    store_state.start()

    pl.semaphore_wait(barrier, PEERS)

    def to_partner(ref, send, recv_):
        return pltpu.make_async_remote_copy(
            src_ref=ref, dst_ref=ref, send_sem=send, recv_sem=recv_,
            device_id=(ep, other), device_id_type=MESH,
        )

    act_copy = to_partner(actx.at[tp], x_send.at[0], x_recv.at[0])
    act_copy.start()
    loads[12].wait()
    loads[13].wait()
    loads[14].wait()
    act_copy.wait()
    a0 = actx[0].astype(F32)
    a1 = actx[1].astype(F32)
    mean_sq = (
        jnp.sum(a0 * a0, axis=1, keepdims=True) + jnp.sum(a1 * a1, axis=1, keepdims=True)
    ) * (1.0 / (2 * CHAN))
    scale = lax.rsqrt(mean_sq + EPS)
    s0 = (a0 * scale * out_gain[:, :CHAN]).astype(BF16)
    s1 = (a1 * scale * out_gain[:, CHAN:]).astype(BF16)
    after = (
        xv[tp].astype(F32) + (mm(s0, out_proj[:CHAN, :]) + mm(s1, out_proj[CHAN:, :]))
    ).astype(BF16)
    outv[...] = after
    after32 = after.astype(F32)
    sqx[tp] = jnp.broadcast_to(jnp.sum(after32 * after32, axis=1, keepdims=True), (SEQ, 128))
    sq_copy = to_partner(sqx.at[tp], x_send.at[1], x_recv.at[1])
    sq_copy.start()
    sq_copy.wait()
    mean_sq = (sqx[0] + sqx[1])[:, :1] * (1.0 / (2 * HALF))
    expert_in = (after32 * lax.rsqrt(mean_sq + EPS) * ffn_gain[tp]).astype(BF16)
    stacked = jnp.concatenate(
        [expert_in[:, q * QW : (q + 1) * QW] for q in range(QUARTERS)], axis=0
    )

    def block_at(ref, p):
        return ref.at[pl.ds(pl.multiple_of(p * ROWS, 8), ROWS)]

    for g in range(GROUPS):
        rows = slice(g * GROWS, (g + 1) * GROWS)
        sendbuf[rows, :] = mm(onehot[rows, :], stacked).astype(BF16)

        def dispatch(j, carry, g=g):
            p = g * GP + j
            pltpu.make_async_remote_copy(
                src_ref=block_at(sendbuf, p), dst_ref=block_at(recv.at[tp], p),
                send_sem=d_send, recv_sem=d_recv.at[g],
                device_id=(peer_of(ZSTEP[g], j, 1), tp), device_id_type=MESH,
            ).start()
            return carry

        lax.fori_loop(1 if g == 0 else 0, GP, dispatch, 0)
    recv[tp, :ROWS, :] = sendbuf[:ROWS, :]

    col = iota((PEERS, ALL), 1)
    spread_t = jnp.where(div_small(col, ROWS) == iota((PEERS, ALL), 0), 1.0, 0.0).astype(BF16)
    c1 = iota((1, ALL), 1)
    c1 = c1 - div_small(c1, ROWS) * ROWS
    cq = div_small(c1, SLOTS)
    cs = (c1 - cq * SLOTS + 1).astype(F32)
    slot_x = mm(slot_tp, spread_t)
    whi_x = mm(whi_tp, spread_t)
    wlo_x = mm(wlo_tp, spread_t)
    hit = slot_x == cs
    for q in range(QUARTERS):
        keep = hit & (cq == q)
        chi[q * SEQ : (q + 1) * SEQ, :] = jnp.where(keep, whi_x, 0.0).astype(BF16)
        clo[q * SEQ : (q + 1) * SEQ, :] = jnp.where(keep, wlo_x, 0.0).astype(BF16)

    loads[15].wait()
    loads[16].wait()
    loads[17].wait()

    def arrived(ref, sem):
        pltpu.make_async_remote_copy(
            src_ref=ref, dst_ref=ref, send_sem=sem, recv_sem=sem,
            device_id=(ep, other), device_id_type=MESH,
        ).wait_recv()

    def group_rows(g):
        first = g * GROWS
        return (first + ROWS, GROWS - ROWS) if g == 0 else (first, GROWS)

    def forward(g):
        first, count = group_rows(g)
        arrived(recv.at[tp, pl.ds(first, count)], d_recv.at[g])
        copy = to_partner(
            recv.at[tp, pl.ds(g * GROWS, GROWS)], f_send.at[g], f_recv.at[g]
        )
        copy.start()
        return copy

    started = []
    for c, chunk in enumerate(CHUNKS):
        copies = [forward(g) for g in chunk]
        started += copies
        first_slot = chunk[0] * GSLOTS
        slots = len(chunk) * GSLOTS
        for copy in copies:
            copy.wait_recv()
        for b in range(len(chunk) * 2):
            r0 = chunk[0] * GROWS + b * BLK
            s0_ = first_slot + b * BSLOTS
            for h in range(2):
                moved = mm(perm[...], recv[h, r0 : r0 + BLK, :]).astype(BF16)
                for q in range(QUARTERS):
                    amat[s0_ : s0_ + BSLOTS, h * HALF + q * QW : h * HALF + (q + 1) * QW] = moved[
                        q * BSLOTS : (q + 1) * BSLOTS, :
                    ]
        srows = slice(first_slot, first_slot + slots)

        def units(n, carry):
            at = pl.ds(pl.multiple_of(n * 256, 256), 256)
            gate = mm(amat[srows, :], wg[:, at])
            up = mm(amat[srows, :], wu[:, at])
            gated = jnp.minimum(gate, LIMIT)
            act = (jnp.clip(up, -LIMIT, LIMIT) + 1.0) * gated * jax.nn.sigmoid(ALPHA * gated)
            hid[srows, at] = act.astype(BF16)
            return carry

        lax.fori_loop(0, 4, units, 0)

        def down_other(n, carry):
            at = pl.ds(pl.multiple_of(n * 256, 256), 256)
            wat = pl.ds(pl.multiple_of(other * HALF + n * 256, 256), 256)
            psend[srows, at] = mm(hid[srows, :], wd[:, wat]).astype(BF16)
            return carry

        lax.fori_loop(0, 4, down_other, 0)
        part_copy = pltpu.make_async_remote_copy(
            src_ref=psend.at[srows], dst_ref=prec.at[srows],
            send_sem=p_send.at[c], recv_sem=p_recv.at[c],
            device_id=(ep, other), device_id_type=MESH,
        )
        part_copy.start()
        started.append(part_copy)

        def down_own(n, carry):
            at = pl.ds(pl.multiple_of(n * 256, 256), 256)
            wat = pl.ds(pl.multiple_of(tp * HALF + n * 256, 256), 256)
            amat[srows, at] = mm(hid[srows, :], wd[:, wat]).astype(BF16)
            return carry

        lax.fori_loop(0, 4, down_own, 0)
        part_copy.wait_recv()
        for i, g in enumerate(chunk):
            for b in range(2):
                s0_ = first_slot + (2 * i + b) * BSLOTS
                total = (
                    amat[s0_ : s0_ + BSLOTS, :HALF].astype(F32)
                    + prec[s0_ : s0_ + BSLOTS, :].astype(F32)
                ).astype(BF16)
                tall = jnp.concatenate(
                    [total[:, q * QW : (q + 1) * QW] for q in range(QUARTERS)], axis=0
                )
                r0 = g * GROWS + b * BLK
                rsend[r0 : r0 + BLK, :] = mm(permt[...], tall).astype(BF16)

            def give_back(j, carry, g=g):
                p = g * GP + j
                pltpu.make_async_remote_copy(
                    src_ref=block_at(rsend, p), dst_ref=block_at(rrecv, p),
                    send_sem=r_send, recv_sem=r_recv.at[g],
                    device_id=(peer_of(ZSTEP[g], j, -1), tp), device_id_type=MESH,
                ).start()
                return carry

            lax.fori_loop(1 if g == 0 else 0, GP, give_back, 0)
            if g == 0:
                rrecv[:ROWS, :] = rsend[:ROWS, :]

    total = jnp.zeros((QUARTERS * SEQ, QW), F32)
    for g in range(GROUPS):
        first, count = group_rows(g)
        arrived(rrecv.at[pl.ds(first, count)], r_recv.at[g])
        rows = slice(g * GROWS, (g + 1) * GROWS)
        got = rrecv[rows, :]
        total = total + mm(chi[:, rows], got) + mm(clo[:, rows], got)
    for q in range(QUARTERS):
        cols = slice(q * QW, (q + 1) * QW)
        outv[:, cols] = (
            outv[:, cols].astype(F32) + total[q * SEQ : (q + 1) * SEQ, :]
        ).astype(BF16)
    store_out = pltpu.make_async_copy(outv, out_ref, out_sems.at[1])
    store_out.start()

    for copy in started:
        copy.wait_send()
    for sem, buf in ((d_send, sendbuf), (r_send, rsend)):
        sent = buf.at[pl.ds(ROWS, ALL - ROWS)]
        pltpu.make_async_remote_copy(
            src_ref=sent, dst_ref=sent, send_sem=sem, recv_sem=sem,
            device_id=(ep, other), device_id_type=MESH,
        ).wait_send()
    store_state.wait()
    store_out.wait()


def local(
    residual,
    route_ids,
    route_weights,
    carried_state,
    mix_gain,
    in_proj,
    decay_rate,
    frequency,
    step_size,
    input_map,
    output_matrix,
    passthrough_scale,
    out_gain,
    out_proj,
    ffn_gain,
    w_gate,
    w_up,
    w_down,
):
    xg = lax.all_gather(residual, "tp", axis=0)
    args = (
        xg,
        route_ids.T,
        route_weights.T,
        carried_state,
        mix_gain.reshape(1, -1),
        in_proj,
        decay_rate,
        frequency,
        step_size.reshape(1, -1),
        jnp.swapaxes(input_map, 2, 3).reshape(2, CHAN, -1),
        output_matrix.reshape(2, CHAN, -1),
        passthrough_scale.reshape(1, -1),
        out_gain.reshape(1, -1),
        out_proj,
        ffn_gain.reshape(2, 1, -1),
        w_gate.reshape(w_gate.shape[1:]),
        w_up.reshape(w_up.shape[1:]),
        w_down.reshape(w_down.shape[1:]),
    )
    dma = pltpu.SemaphoreType.DMA
    vmem = pltpu.VMEM
    updated, new_state = pl.pallas_call(
        kernel,
        out_shape=(
            jax.ShapeDtypeStruct(residual.shape, BF16),
            jax.ShapeDtypeStruct(carried_state.shape, F32),
        ),
        in_specs=[pl.BlockSpec(memory_space=pl.ANY)] * len(args),
        out_specs=(pl.BlockSpec(memory_space=pl.ANY),) * 2,
        scratch_shapes=[vmem(a.shape, a.dtype) for a in args]
        + [
            vmem((SEQ, HALF), BF16),
            vmem(carried_state.shape, F32),
            vmem((2, SEQ, CHAN), BF16),
            vmem((2, SEQ, 128), F32),
            vmem((ALL, QUARTERS * SEQ), BF16),
            vmem((QUARTERS * SEQ, ALL), BF16),
            vmem((QUARTERS * SEQ, ALL), BF16),
            vmem((BLK, BLK), BF16),
            vmem((BLK, BLK), BF16),
            vmem((PAD, QW), BF16),
            vmem((2, PAD, QW), BF16),
            vmem((PAD, QW), BF16),
            vmem((PAD, QW), BF16),
            vmem((PEERS * SLOTS, 2 * HALF), BF16),
            vmem((PEERS * SLOTS, HALF), BF16),
            vmem((PEERS * SLOTS, HALF), BF16),
            vmem((PEERS * SLOTS, HALF), BF16),
            dma((len(args),)),
            dma((2,)),
            dma((2,)),
            dma((2,)),
            dma,
            dma((GROUPS,)),
            dma((GROUPS,)),
            dma((GROUPS,)),
            dma((len(CHUNKS),)),
            dma((len(CHUNKS),)),
            dma,
            dma((GROUPS,)),
        ],
        compiler_params=pltpu.CompilerParams(
            collective_id=0, has_side_effects=True, vmem_limit_bytes=60 * 1024 * 1024
        ),
    )(*args)
    return updated, new_state


def solution(mesh):
    placed = (
        P("ep", "tp"),
        P("ep", None),
        P("ep", None),
        P(None, "ep", "tp"),
        P(),
        P(None, "tp"),
        P("tp", None),
        P("tp", None),
        P("tp"),
        P(None, "tp", None, None),
        P(None, "tp", None, None),
        P("tp"),
        P(),
        P(None, "tp"),
        P(),
        P("ep", None, "tp"),
        P("ep", None, "tp"),
        P("ep", "tp", None),
    )
    return jax.shard_map(
        local,
        mesh=mesh,
        in_specs=placed,
        out_specs=(P("ep", "tp"), P(None, "ep", "tp")),
        check_vma=False,
    )
```

```python
import jax
import jax.numpy as jnp
from jax import lax
from jax.experimental import pallas as pl
from jax.experimental.pallas import tpu as pltpu
from jax.sharding import PartitionSpec as P

F32 = jnp.float32
BF16 = jnp.bfloat16
MESH = pl.DeviceIdType.MESH

VMEM_LIMIT = 62 * 1024 * 1024
EPS = 1e-06
LIMIT = 7.0
ALPHA = 1.702

SEQ = 64
HALF = 1024
STATES = 2048
CHAN = 512
PEERS = 64
SLOTS = 6
QUARTERS = 4
QW = HALF // QUARTERS
ROWS = SLOTS * QUARTERS
ALL = PEERS * ROWS
PAD = ALL + 8
OWN = ALL - ROWS
GROUPS = 8
GP = PEERS // GROUPS
GROWS = GP * ROWS
GSLOTS = GP * SLOTS
CHUNKS = ((0, 1, 2), (3, 4, 5), (6, 7))


def hops(step):
    return sum(min(d, 4 - d) for d in step)


STEPS = sorted(
    ((dz, dy, dx) for dz in range(4) for dy in range(4) for dx in range(4)), key=hops, reverse=True
)

NT = (((1,), (1,)), ((), ()))


def mm(a, b):
    return jnp.dot(a, b, preferred_element_type=F32)


def mm_nt(a, b):
    return lax.dot_general(a, b, NT, preferred_element_type=F32)


def iota(shape, dim):
    return lax.broadcasted_iota(jnp.int32, shape, dim)


def div_small(v, d):
    return ((v.astype(F32) + 0.5) * (1.0 / d)).astype(jnp.int32)


def kernel(
    x_in,
    ids_in,
    wts_in,
    decay_in,
    freq_in,
    step_in,
    imap_in,
    omap_in,
    mix_gain_in,
    in_proj_in,
    state_in,
    pscale_in,
    out_gain_in,
    out_proj_in,
    ffn_gain_in,
    wg_in,
    wu_in,
    wd_in,
    out_ref,
    nstate_ref,
    outv,
    nstate,
    xv,
    ids,
    wts,
    decay,
    freq,
    step,
    imap,
    omap,
    mix_gain,
    in_proj,
    state,
    pscale,
    out_gain,
    out_proj,
    ffn_gain,
    wg,
    wu,
    wd,
    inmix,
    outmix,
    actx,
    sqx,
    onehot,
    chi,
    clo,
    perm,
    permt,
    sendbuf,
    recv,
    rsend,
    rrecv,
    amat,
    hid,
    psend,
    prec,
    in_sems,
    out_sems,
    x_send,
    x_recv,
    d_send,
    d_recv,
    f_send,
    f_recv,
    p_send,
    p_recv,
    r_send,
    r_recv,
):
    ep = lax.axis_index("ep")
    tp = lax.axis_index("tp")
    other = 1 - tp
    z = lax.div(ep, 16)
    y = lax.rem(lax.div(ep, 4), 4)
    x = lax.rem(ep, 4)
    z_at = [lax.rem(z + d, 4) * 16 for d in range(4)]
    y_at = [lax.rem(y + d, 4) * 4 for d in range(4)]
    x_at = [lax.rem(x + d, 4) for d in range(4)]

    def peer_of(p, sign):
        dz, dy, dx = STEPS[p]
        return z_at[sign * dz % 4] + y_at[sign * dy % 4] + x_at[sign * dx % 4]

    barrier = pltpu.get_barrier_semaphore()
    pl.semaphore_signal(barrier, inc=1, device_id=(ep, other), device_id_type=MESH)

    def greet(i, carry):
        pl.semaphore_signal(
            barrier, inc=1, device_id=(lax.rem(ep + i, PEERS), tp), device_id_type=MESH
        )
        return carry

    lax.fori_loop(1, PEERS, greet, 0)

    pairs = (
        (x_in, xv.at[tp]),
        (ids_in, ids),
        (wts_in, wts),
        (decay_in, decay),
        (freq_in, freq),
        (step_in, step),
        (imap_in, imap),
        (omap_in, omap),
        (mix_gain_in, mix_gain),
        (in_proj_in, in_proj),
        (state_in, state),
        (pscale_in, pscale),
        (out_gain_in, out_gain),
        (out_proj_in, out_proj),
        (ffn_gain_in, ffn_gain),
        (wg_in, wg),
        (wu_in, wu),
        (wd_in, wd),
    )
    loads = [pltpu.make_async_copy(a, b, in_sems.at[i]) for i, (a, b) in enumerate(pairs)]
    for load in loads:
        load.start()

    loads[1].wait()
    loads[2].wait()
    expert = iota((PEERS, SEQ), 0)
    named = jnp.zeros((PEERS, SEQ), F32)
    weight = jnp.zeros((PEERS, SEQ), F32)
    for k in range(4):
        hit = ids[k : k + 1, :] == expert
        named = named + jnp.where(hit, 1.0, 0.0)
        weight = weight + jnp.where(hit, wts[k : k + 1, :], 0.0)
    earlier = jnp.where(iota((SEQ, SEQ), 0) < iota((SEQ, SEQ), 1), 1.0, 0.0).astype(BF16)
    slot_of = named * (mm(named.astype(BF16), earlier) + 1.0)
    pos = iota((PEERS, PEERS), 0)
    named_at = jnp.zeros((PEERS, PEERS), jnp.int32)
    for p in range(PEERS):
        named_at = jnp.where(pos == p, peer_of(p, 1), named_at)
    order = jnp.where(named_at == iota((PEERS, PEERS), 1), 1.0, 0.0).astype(BF16)
    w_hi = weight.astype(BF16)
    w_lo = (weight - w_hi.astype(F32)).astype(BF16)
    slot_pt = mm(order, slot_of.astype(BF16)).astype(BF16)
    eye = jnp.where(iota((SEQ, SEQ), 0) == iota((SEQ, SEQ), 1), 1.0, 0.0).astype(BF16)

    def turned(v):
        return mm_nt(eye, v).astype(BF16)

    slot_tp = turned(slot_pt)
    whi_tp = turned(mm(order, w_hi).astype(BF16))
    wlo_tp = turned(mm(order, w_lo).astype(BF16))

    slot_p4 = jnp.concatenate([slot_pt] * QUARTERS, axis=1)
    row = iota((GROWS, QUARTERS * SEQ), 0)
    rowp = div_small(row, ROWS)
    rem_row = row - rowp * ROWS
    rowq = div_small(rem_row, SLOTS)
    rows_ = rem_row - rowq * SLOTS
    want = jnp.where(rowq == (iota((GROWS, QUARTERS * SEQ), 1) >> 6), rows_ + 1, -1).astype(F32)
    spread_row = div_small(iota((GROWS, PEERS), 0), ROWS)
    spread_col = iota((GROWS, PEERS), 1)
    for b in range(GROUPS):
        spread = jnp.where(spread_row + b * 8 == spread_col, 1.0, 0.0).astype(BF16)
        onehot[b * GROWS : (b + 1) * GROWS, :] = jnp.where(
            mm(spread, slot_p4) == want, 1.0, 0.0
        ).astype(BF16)

    def block_perm(rdim, cdim):
        r = iota((GROWS, GROWS), rdim)
        c = iota((GROWS, GROWS), cdim)
        rq = div_small(r, GSLOTS)
        rr = r - rq * GSLOTS
        rp = div_small(rr, SLOTS)
        rs = rr - rp * SLOTS
        return jnp.where(rp * ROWS + rq * SLOTS + rs == c, 1.0, 0.0).astype(BF16)

    perm[...] = block_perm(0, 1)
    permt[...] = block_perm(1, 0)

    loads[3].wait()
    loads[4].wait()
    loads[5].wait()
    rate_real = -decay[...]
    rate_imag = freq[...]
    n_groups, n_state = rate_real.shape
    diag = iota((n_groups, n_groups), 0) == iota((n_groups, n_groups), 1)
    time_step = jnp.sum(jnp.where(diag, step[...], 0.0), axis=1, keepdims=True)
    magnitude = jnp.exp(rate_real * time_step)
    phase = rate_imag * time_step
    bar_real = magnitude * jnp.cos(phase)
    bar_imag = magnitude * jnp.sin(phase)
    denominator = rate_real * rate_real + rate_imag * rate_imag
    shifted = bar_real - 1.0
    coef_real = (shifted * rate_real + bar_imag * rate_imag) / denominator
    coef_imag = (bar_imag * rate_real - shifted * rate_imag) / denominator
    own_group = iota((n_groups, STATES), 0) == (iota((n_groups, STATES), 1) >> 6)

    def as_row(v):
        wide = jnp.concatenate([v] * (STATES // n_state), axis=1)
        return jnp.sum(jnp.where(own_group, wide, 0.0), axis=0, keepdims=True)

    bar_real, bar_imag, coef_real, coef_imag = (
        as_row(v) for v in (bar_real, bar_imag, coef_real, coef_imag)
    )

    same = (iota((128, 512), 0) >> 4) == (iota((128, 512), 1) >> 6)

    def spread_groups(m):
        return jnp.where(same, jnp.concatenate([m] * 8, axis=1), 0.0).astype(BF16)

    loads[6].wait()
    loads[7].wait()
    for b in range(4):
        rows = slice(b * 128, (b + 1) * 128)
        for i in range(2):
            inmix[i, rows, :] = spread_groups(imap[i, rows, :])
        outmix[0, rows, :] = spread_groups(omap[0, rows, :])
        outmix[1, rows, :] = spread_groups(-omap[1, rows, :])

    loads[0].wait()
    pl.semaphore_wait(barrier, PEERS)

    def to_partner(ref, send, recv_):
        return pltpu.make_async_remote_copy(
            src_ref=ref, dst_ref=ref, send_sem=send, recv_sem=recv_,
            device_id=(ep, other), device_id_type=MESH,
        )

    x_copy = to_partner(xv.at[tp], x_send.at[2], x_recv.at[2])
    x_copy.start()
    loads[10].wait()
    for b in range(4):
        cols = slice(b * 512, (b + 1) * 512)
        hr = state[0, :, cols]
        hi = state[1, :, cols]
        br, bi = bar_real[:, cols], bar_imag[:, cols]
        nstate[0, :, cols] = br * hr - bi * hi
        nstate[1, :, cols] = br * hi + bi * hr
    loads[8].wait()
    loads[9].wait()
    loads[11].wait()
    x_copy.wait()
    x0 = xv[0].astype(F32)
    x1 = xv[1].astype(F32)
    mean_sq = (
        jnp.sum(x0 * x0, axis=1, keepdims=True) + jnp.sum(x1 * x1, axis=1, keepdims=True)
    ) * (1.0 / (2 * HALF))
    scale = lax.rsqrt(mean_sq + EPS)
    n0 = (x0 * scale * mix_gain[:, :HALF]).astype(BF16)
    n1 = (x1 * scale * mix_gain[:, HALF:]).astype(BF16)
    channels = (mm(n0, in_proj[:HALF, :]) + mm(n1, in_proj[HALF:, :])).astype(BF16)
    for b in range(4):
        rows = slice(b * 128, (b + 1) * 128)
        cols = slice(b * 512, (b + 1) * 512)
        ch = channels[:, rows]
        u0 = mm(ch, inmix[0, rows, :])
        u1 = mm(ch, inmix[1, rows, :])
        cr, ci = coef_real[:, cols], coef_imag[:, cols]
        nr = nstate[0, :, cols] + (cr * u0 - ci * u1)
        ni = nstate[1, :, cols] + (cr * u1 + ci * u0)
        nstate[0, :, cols] = nr
        nstate[1, :, cols] = ni
        mixed = (
            mm_nt(nr.astype(BF16), outmix[0, rows, :])
            + mm_nt(ni.astype(BF16), outmix[1, rows, :])
            + pscale[:, rows] * ch.astype(F32)
        )
        actx[tp, :, rows] = jax.nn.gelu(mixed, approximate=True).astype(BF16)

    store_state = pltpu.make_async_copy(nstate, nstate_ref, out_sems.at[0])
    store_state.start()
    act_copy = to_partner(actx.at[tp], x_send.at[0], x_recv.at[0])
    act_copy.start()
    loads[12].wait()
    loads[13].wait()
    loads[14].wait()
    act_copy.wait()
    a0 = actx[0].astype(F32)
    a1 = actx[1].astype(F32)
    mean_sq = (
        jnp.sum(a0 * a0, axis=1, keepdims=True) + jnp.sum(a1 * a1, axis=1, keepdims=True)
    ) * (1.0 / (2 * CHAN))
    scale = lax.rsqrt(mean_sq + EPS)
    s0 = (a0 * scale * out_gain[:, :CHAN]).astype(BF16)
    s1 = (a1 * scale * out_gain[:, CHAN:]).astype(BF16)
    after = (
        xv[tp].astype(F32) + (mm(s0, out_proj[:CHAN, :]) + mm(s1, out_proj[CHAN:, :]))
    ).astype(BF16)
    outv[...] = after
    after32 = after.astype(F32)
    sqx[tp] = jnp.broadcast_to(jnp.sum(after32 * after32, axis=1, keepdims=True), (SEQ, 128))
    sq_copy = to_partner(sqx.at[tp], x_send.at[1], x_recv.at[1])
    sq_copy.start()
    sq_copy.wait()
    mean_sq = (sqx[0] + sqx[1])[:, :1] * (1.0 / (2 * HALF))
    expert_in = (after32 * lax.rsqrt(mean_sq + EPS) * ffn_gain[tp]).astype(BF16)
    stacked = jnp.concatenate(
        [expert_in[:, q * QW : (q + 1) * QW] for q in range(QUARTERS)], axis=0
    )

    def send_block(src, dst, p, sign, send, recv_):
        at = pl.ds(p * ROWS, ROWS)
        pltpu.make_async_remote_copy(
            src_ref=src.at[at], dst_ref=dst.at[at], send_sem=send, recv_sem=recv_,
            device_id=(peer_of(p, sign), tp), device_id_type=MESH,
        ).start()

    for b in range(4):
        rows = slice(b * 2 * GROWS, (b + 1) * 2 * GROWS)
        sendbuf[rows, :] = mm(onehot[rows, :], stacked).astype(BF16)
        for p in range(b * 2 * GP, min((b + 1) * 2 * GP, PEERS - 1)):
            send_block(sendbuf, recv.at[tp], p, 1, d_send, d_recv.at[p // GP])
    recv[tp, OWN:ALL, :] = sendbuf[OWN:ALL, :]

    col = iota((PEERS, ALL), 1)
    spread_t = jnp.where(div_small(col, ROWS) == iota((PEERS, ALL), 0), 1.0, 0.0).astype(BF16)
    c1 = iota((1, ALL), 1)
    c1 = c1 - div_small(c1, ROWS) * ROWS
    cq = div_small(c1, SLOTS)
    cs = (c1 - cq * SLOTS + 1).astype(F32)
    slot_x = mm(slot_tp, spread_t)
    whi_x = mm(whi_tp, spread_t)
    wlo_x = mm(wlo_tp, spread_t)
    hit = slot_x == cs
    for q in range(QUARTERS):
        keep = hit & (cq == q)
        chi[q * SEQ : (q + 1) * SEQ, :] = jnp.where(keep, whi_x, 0.0).astype(BF16)
        clo[q * SEQ : (q + 1) * SEQ, :] = jnp.where(keep, wlo_x, 0.0).astype(BF16)

    loads[15].wait()
    loads[16].wait()
    loads[17].wait()

    def arrived(ref, sem):
        pltpu.make_async_remote_copy(
            src_ref=ref, dst_ref=ref, send_sem=sem, recv_sem=sem,
            device_id=(ep, other), device_id_type=MESH,
        ).wait_recv()

    started = []
    forwards = [None] * GROUPS

    def forward(g):
        first = g * GROWS
        count = min(GROWS, OWN - first)
        arrived(recv.at[tp, pl.ds(first, count)], d_recv.at[g])
        copy = to_partner(recv.at[tp, pl.ds(first, GROWS)], f_send.at[g], f_recv.at[g])
        copy.start()
        started.append(copy)
        forwards[g] = copy

    def assemble(g):
        forwards[g].wait_recv()
        slots = slice(g * GSLOTS, (g + 1) * GSLOTS)
        for h in range(2):
            moved = mm(perm[...], recv[h, g * GROWS : (g + 1) * GROWS, :]).astype(BF16)
            for q in range(QUARTERS):
                amat[slots, h * HALF + q * QW : h * HALF + (q + 1) * QW] = moved[
                    q * GSLOTS : (q + 1) * GSLOTS, :
                ]

    for g in CHUNKS[0]:
        forward(g)
    for g in CHUNKS[0]:
        assemble(g)
    for c, chunk in enumerate(CHUNKS):
        following = CHUNKS[c + 1] if c + 1 < len(CHUNKS) else ()
        srows = slice(chunk[0] * GSLOTS, (chunk[-1] + 1) * GSLOTS)
        lhs = amat[srows, :]
        for n in range(2):
            at = slice(n * 512, (n + 1) * 512)
            gate = mm(lhs, wg[:, at])
            up = mm(lhs, wu[:, at])
            gated = jnp.minimum(gate, LIMIT)
            act = (jnp.clip(up, -LIMIT, LIMIT) + 1.0) * gated * jax.nn.sigmoid(ALPHA * gated)
            hid[srows, at] = act.astype(BF16)
        for g in following:
            forward(g)
        lhs = hid[srows, :]
        for n in range(2):
            wat = pl.ds(pl.multiple_of(other * HALF + n * 512, 512), 512)
            psend[srows, n * 512 : (n + 1) * 512] = mm(lhs, wd[:, wat]).astype(BF16)
        part_copy = pltpu.make_async_remote_copy(
            src_ref=psend.at[srows], dst_ref=prec.at[srows],
            send_sem=p_send.at[c], recv_sem=p_recv.at[c],
            device_id=(ep, other), device_id_type=MESH,
        )
        part_copy.start()
        started.append(part_copy)
        for n in range(2):
            wat = pl.ds(pl.multiple_of(tp * HALF + n * 512, 512), 512)
            amat[srows, n * 512 : (n + 1) * 512] = mm(lhs, wd[:, wat]).astype(BF16)
        for g in following:
            assemble(g)
        part_copy.wait_recv()
        for g in chunk:
            slots = slice(g * GSLOTS, (g + 1) * GSLOTS)
            both = (amat[slots, :HALF].astype(F32) + prec[slots, :].astype(F32)).astype(BF16)
            tall = jnp.concatenate(
                [both[:, q * QW : (q + 1) * QW] for q in range(QUARTERS)], axis=0
            )
            rsend[g * GROWS : (g + 1) * GROWS, :] = mm(permt[...], tall).astype(BF16)
            for p in range(g * GP, min((g + 1) * GP, PEERS - 1)):
                send_block(rsend, rrecv, p, -1, r_send, r_recv.at[c])
    rrecv[OWN:ALL, :] = rsend[OWN:ALL, :]

    total = jnp.zeros((QUARTERS * SEQ, QW), F32)
    for c, chunk in enumerate(CHUNKS):
        first = chunk[0] * GROWS
        last = (chunk[-1] + 1) * GROWS
        arrived(rrecv.at[pl.ds(first, min(last, OWN) - first)], r_recv.at[c])
        got = rrecv[first:last, :]
        total = total + mm(chi[:, first:last], got) + mm(clo[:, first:last], got)
    for q in range(QUARTERS):
        cols = slice(q * QW, (q + 1) * QW)
        outv[:, cols] = (
            outv[:, cols].astype(F32) + total[q * SEQ : (q + 1) * SEQ, :]
        ).astype(BF16)
    store_out = pltpu.make_async_copy(outv, out_ref, out_sems.at[1])
    store_out.start()
    for copy in started:
        copy.wait_send()
    for sem, buf in ((d_send, sendbuf), (r_send, rsend)):
        sent = buf.at[pl.ds(0, OWN)]
        pltpu.make_async_remote_copy(
            src_ref=sent, dst_ref=sent, send_sem=sem, recv_sem=sem,
            device_id=(ep, other), device_id_type=MESH,
        ).wait_send()
    store_state.wait()
    store_out.wait()


def store(u_in, s_in, u_out, s_out, u_buf, s_buf, in_sems, out_sems):
    pieces = [
        (s_in.at[i, pl.ds(r, 32)], s_buf.at[i, pl.ds(r, 32)], s_out.at[i, pl.ds(r, 32)])
        for i in range(2)
        for r in range(0, SEQ, 32)
    ]
    pieces.append((u_in, u_buf, u_out))
    loads = [pltpu.make_async_copy(a, b, in_sems.at[i]) for i, (a, b, _) in enumerate(pieces)]
    stores = [pltpu.make_async_copy(b, c, out_sems.at[i]) for i, (_, b, c) in enumerate(pieces)]
    for load in loads:
        load.start()
    for load, put in zip(loads, stores):
        load.wait()
        put.start()
    for put in stores:
        put.wait()


def local(
    residual,
    route_ids,
    route_weights,
    carried_state,
    mix_gain,
    in_proj,
    decay_rate,
    frequency,
    step_size,
    input_map,
    output_matrix,
    passthrough_scale,
    out_gain,
    out_proj,
    ffn_gain,
    w_gate,
    w_up,
    w_down,
):
    args = (
        residual,
        route_ids.T,
        route_weights.T,
        decay_rate,
        frequency,
        step_size.reshape(1, -1),
        jnp.swapaxes(input_map, 2, 3).reshape(2, CHAN, -1),
        output_matrix.reshape(2, CHAN, -1),
        mix_gain.reshape(1, -1),
        in_proj,
        carried_state,
        passthrough_scale.reshape(1, -1),
        out_gain.reshape(1, -1),
        out_proj,
        ffn_gain.reshape(2, 1, -1),
        w_gate.reshape(w_gate.shape[1:]),
        w_up.reshape(w_up.shape[1:]),
        w_down.reshape(w_down.shape[1:]),
    )
    dma = pltpu.SemaphoreType.DMA
    vmem = pltpu.VMEM
    out_shape = (
        jax.ShapeDtypeStruct(residual.shape, BF16),
        jax.ShapeDtypeStruct(carried_state.shape, F32),
    )
    results = pl.pallas_call(
        kernel,
        out_shape=out_shape,
        in_specs=[pl.BlockSpec(memory_space=pl.ANY)] * len(args),
        out_specs=(pl.BlockSpec(memory_space=pl.ANY),) * 2,
        scratch_shapes=[
            vmem(residual.shape, BF16),
            vmem(carried_state.shape, F32),
            vmem((2, *residual.shape), BF16),
        ]
        + [vmem(a.shape, a.dtype) for a in args[1:]]
        + [
            vmem((2, CHAN, 512), BF16),
            vmem((2, CHAN, 512), BF16),
            vmem((2, SEQ, CHAN), BF16),
            vmem((2, SEQ, 128), F32),
            vmem((ALL, QUARTERS * SEQ), BF16),
            vmem((QUARTERS * SEQ, ALL), BF16),
            vmem((QUARTERS * SEQ, ALL), BF16),
            vmem((GROWS, GROWS), BF16),
            vmem((GROWS, GROWS), BF16),
            vmem((PAD, QW), BF16),
            vmem((2, PAD, QW), BF16),
            vmem((PAD, QW), BF16),
            vmem((PAD, QW), BF16),
            vmem((PEERS * SLOTS, 2 * HALF), BF16),
            vmem((PEERS * SLOTS, HALF), BF16),
            vmem((PEERS * SLOTS, HALF), BF16),
            vmem((PEERS * SLOTS, HALF), BF16),
            dma((len(args),)),
            dma((2,)),
            dma((3,)),
            dma((3,)),
            dma,
            dma((GROUPS,)),
            dma((GROUPS,)),
            dma((GROUPS,)),
            dma((len(CHUNKS),)),
            dma((len(CHUNKS),)),
            dma,
            dma((len(CHUNKS),)),
        ],
        compiler_params=pltpu.CompilerParams(
            collective_id=0, has_side_effects=True, vmem_limit_bytes=VMEM_LIMIT
        ),
    )(*args)
    return pl.pallas_call(
        store,
        out_shape=out_shape,
        in_specs=[pl.BlockSpec(memory_space=pl.ANY)] * 2,
        out_specs=(pl.BlockSpec(memory_space=pl.ANY),) * 2,
        scratch_shapes=[
            vmem(residual.shape, BF16),
            vmem(carried_state.shape, F32),
            dma((5,)),
            dma((5,)),
        ],
        compiler_params=pltpu.CompilerParams(vmem_limit_bytes=VMEM_LIMIT),
    )(*results)


def solution(mesh):
    placed = (
        P("ep", "tp"),
        P("ep", None),
        P("ep", None),
        P(None, "ep", "tp"),
        P(),
        P(None, "tp"),
        P("tp", None),
        P("tp", None),
        P("tp"),
        P(None, "tp", None, None),
        P(None, "tp", None, None),
        P("tp"),
        P(),
        P(None, "tp"),
        P(),
        P("ep", None, "tp"),
        P("ep", None, "tp"),
        P("ep", "tp", None),
    )
    return jax.shard_map(
        local,
        mesh=mesh,
        in_specs=placed,
        out_specs=(P("ep", "tp"), P(None, "ep", "tp")),
        check_vma=False,
    )
```

```python
import jax
import jax.numpy as jnp
from jax import lax
from jax.experimental import pallas as pl
from jax.experimental.pallas import tpu as pltpu
from jax.sharding import PartitionSpec as P

F32 = jnp.float32
BF16 = jnp.bfloat16
MESH = pl.DeviceIdType.MESH

VMEM_LIMIT = 62 * 1024 * 1024
EPS = 1e-06
LIMIT = 7.0
ALPHA = 1.702

SEQ = 64
HALF = 1024
STATES = 2048
CHAN = 512
PEERS = 64
SLOTS = 6
QUARTERS = 4
QW = HALF // QUARTERS
ROWS = SLOTS * QUARTERS
ALL = PEERS * ROWS
PAD = ALL + 8
OWN = ALL - ROWS
GROUPS = 8
GP = PEERS // GROUPS
GROWS = GP * ROWS
GSLOTS = GP * SLOTS
CHUNKS = ((0, 1), (2, 3, 4), (5, 6, 7))
UNITS = ((0,), (1,), (2, 3, 4), (5, 6, 7))

UNIT_OF = {g: u for u, unit in enumerate(UNITS) for g in unit}


def hops(step):
    return sum(min(d, 4 - d) for d in step)


STEPS = sorted(
    ((dz, dy, dx) for dz in range(4) for dy in range(4) for dx in range(4)), key=hops, reverse=True
)

NT = (((1,), (1,)), ((), ()))


def mm(a, b):
    return jnp.dot(a, b, preferred_element_type=F32)


def mm_nt(a, b):
    return lax.dot_general(a, b, NT, preferred_element_type=F32)


def iota(shape, dim):
    return lax.broadcasted_iota(jnp.int32, shape, dim)


def div_small(v, d):
    return ((v.astype(F32) + 0.5) * (1.0 / d)).astype(jnp.int32)


def kernel(
    x_in,
    ids_in,
    wts_in,
    decay_in,
    freq_in,
    step_in,
    imap_in,
    omap_in,
    mix_gain_in,
    in_proj_in,
    state_in,
    pscale_in,
    out_gain_in,
    out_proj_in,
    ffn_gain_in,
    wg_in,
    wu_in,
    wd_in,
    out_ref,
    nstate_ref,
    outv,
    nstate,
    xv,
    ids,
    wts,
    rates,
    step,
    maps,
    mix_gain,
    in_proj,
    state,
    pscale,
    out_gain,
    out_proj,
    ffn_gain,
    wgu,
    wd,
    inmix,
    outmix,
    actx,
    sqx,
    onehot,
    chi,
    clo,
    perm,
    permt,
    sendbuf,
    recv,
    rsend,
    rrecv,
    amat,
    hid,
    psend,
    prec,
    local_sems,
    hello,
    x_recv,
    d_recv,
    f_recv,
    p_recv,
    r_recv,
):
    ep = lax.axis_index("ep")
    tp = lax.axis_index("tp")
    other = 1 - tp
    z = lax.div(ep, 16)
    y = lax.rem(lax.div(ep, 4), 4)
    x = lax.rem(ep, 4)
    z_at = [lax.rem(z + d, 4) * 16 for d in range(4)]
    y_at = [lax.rem(y + d, 4) * 4 for d in range(4)]
    x_at = [lax.rem(x + d, 4) for d in range(4)]

    def peer_of(p, sign):
        dz, dy, dx = STEPS[p]
        return z_at[sign * dz % 4] + y_at[sign * dy % 4] + x_at[sign * dx % 4]

    pairs = (
        (x_in, xv.at[tp], 0),
        (decay_in, rates.at[0], 1),
        (freq_in, rates.at[1], 1),
        (step_in, step, 2),
        (imap_in, maps.at[0], 3),
        (omap_in, maps.at[1], 3),
        (state_in, state, 4),
        (in_proj_in, in_proj, 5),
        (mix_gain_in, mix_gain, 6),
        (pscale_in, pscale, 7),
        (ids_in, ids, 8),
        (wts_in, wts, 9),
        (out_gain_in, out_gain, 10),
        (out_proj_in, out_proj, 11),
        (ffn_gain_in, ffn_gain, 12),
        (wg_in, wgu.at[0], 0),
        (wu_in, wgu.at[1], 0),
        (wd_in, wd, 1),
    )

    def loaded(ref, sem):
        pltpu.make_async_copy(ref, ref, local_sems.at[sem]).wait()

    loads = [pltpu.make_async_copy(a, b, local_sems.at[i]) for a, b, i in pairs]
    loads[0].start()
    barrier = pltpu.get_barrier_semaphore()

    @pl.when(tp == 0)
    def _():
        pl.semaphore_signal(barrier, inc=1, device_id=(ep, other), device_id_type=MESH)

    for load in loads[1:15]:
        load.start()

    @pl.when(tp == 1)
    def _():
        pl.semaphore_wait(barrier, 1)
        pl.semaphore_signal(hello, inc=1, device_id=(ep, other), device_id_type=MESH)

    @pl.when(tp == 0)
    def _():
        pl.semaphore_wait(hello, 1)

        def greet(i, carry):
            pl.semaphore_signal(
                barrier, inc=1, device_id=(lax.rem(ep + i, PEERS), tp), device_id_type=MESH
            )
            return carry

        lax.fori_loop(1, PEERS, greet, 0)


    loaded(xv.at[tp], 0)

    def to_partner(ref, send, recv_):
        return pltpu.make_async_remote_copy(
            src_ref=ref, dst_ref=ref, send_sem=send, recv_sem=recv_,
            device_id=(ep, other), device_id_type=MESH,
        )

    x_copy = to_partner(xv.at[tp], local_sems.at[0], x_recv.at[2])
    x_copy.start()

    loaded(rates, 1)
    loaded(step, 2)
    rate_real = -rates[0]
    rate_imag = rates[1]
    n_groups, n_state = rate_real.shape
    diag = iota((n_groups, n_groups), 0) == iota((n_groups, n_groups), 1)
    time_step = jnp.sum(jnp.where(diag, step[...], 0.0), axis=1, keepdims=True)
    magnitude = jnp.exp(rate_real * time_step)
    phase = rate_imag * time_step
    bar_real = magnitude * jnp.cos(phase)
    bar_imag = magnitude * jnp.sin(phase)
    denominator = rate_real * rate_real + rate_imag * rate_imag
    shifted = bar_real - 1.0
    coef_real = (shifted * rate_real + bar_imag * rate_imag) / denominator
    coef_imag = (bar_imag * rate_real - shifted * rate_imag) / denominator
    own_group = iota((n_groups, STATES), 0) == (iota((n_groups, STATES), 1) >> 6)

    def as_row(v):
        wide = jnp.concatenate([v] * (STATES // n_state), axis=1)
        return jnp.sum(jnp.where(own_group, wide, 0.0), axis=0, keepdims=True)

    bar_real, bar_imag, coef_real, coef_imag = (
        as_row(v) for v in (bar_real, bar_imag, coef_real, coef_imag)
    )

    same = (iota((128, 512), 0) >> 4) == (iota((128, 512), 1) >> 6)

    def spread_groups(m):
        return jnp.where(same, jnp.concatenate([m] * 8, axis=1), 0.0).astype(BF16)

    loaded(maps, 3)
    for b in range(4):
        rows = slice(b * 128, (b + 1) * 128)
        for i in range(2):
            inmix[i, rows, :] = spread_groups(maps[0, i, rows, :])
        outmix[0, rows, :] = spread_groups(maps[1, 0, rows, :])
        outmix[1, rows, :] = spread_groups(-maps[1, 1, rows, :])

    loaded(state, 4)
    for b in range(4):
        cols = slice(b * 512, (b + 1) * 512)
        hr = state[0, :, cols]
        hi = state[1, :, cols]
        br, bi = bar_real[:, cols], bar_imag[:, cols]
        nstate[0, :, cols] = br * hr - bi * hi
        nstate[1, :, cols] = br * hi + bi * hr
    loaded(in_proj, 5)
    loaded(mix_gain, 6)
    loaded(pscale, 7)
    x_copy.wait()
    x0 = xv[0].astype(F32)
    x1 = xv[1].astype(F32)
    mean_sq = (
        jnp.sum(x0 * x0, axis=1, keepdims=True) + jnp.sum(x1 * x1, axis=1, keepdims=True)
    ) * (1.0 / (2 * HALF))
    scale = lax.rsqrt(mean_sq + EPS)
    n0 = (x0 * scale * mix_gain[:, :HALF]).astype(BF16)
    n1 = (x1 * scale * mix_gain[:, HALF:]).astype(BF16)
    for load in loads[15:]:
        load.start()
    channels = (mm(n0, in_proj[:HALF, :]) + mm(n1, in_proj[HALF:, :])).astype(BF16)
    for b in range(4):
        rows = slice(b * 128, (b + 1) * 128)
        cols = slice(b * 512, (b + 1) * 512)
        ch = channels[:, rows]
        u0 = mm(ch, inmix[0, rows, :])
        u1 = mm(ch, inmix[1, rows, :])
        cr, ci = coef_real[:, cols], coef_imag[:, cols]
        nr = nstate[0, :, cols] + (cr * u0 - ci * u1)
        ni = nstate[1, :, cols] + (cr * u1 + ci * u0)
        nstate[0, :, cols] = nr
        nstate[1, :, cols] = ni
        mixed = (
            mm_nt(nr.astype(BF16), outmix[0, rows, :])
            + mm_nt(ni.astype(BF16), outmix[1, rows, :])
            + pscale[:, rows] * ch.astype(F32)
        )
        actx[tp, :, rows] = jax.nn.gelu(mixed, approximate=True).astype(BF16)

    store_state = pltpu.make_async_copy(nstate, nstate_ref, local_sems.at[5])
    store_state.start()
    act_copy = to_partner(actx.at[tp], local_sems.at[3], x_recv.at[0])
    act_copy.start()

    loaded(ids, 8)
    loaded(wts, 9)
    expert = iota((PEERS, SEQ), 0)
    named = jnp.zeros((PEERS, SEQ), F32)
    weight = jnp.zeros((PEERS, SEQ), F32)
    for k in range(4):
        hit = ids[k : k + 1, :] == expert
        named = named + jnp.where(hit, 1.0, 0.0)
        weight = weight + jnp.where(hit, wts[k : k + 1, :], 0.0)
    earlier = jnp.where(iota((SEQ, SEQ), 0) < iota((SEQ, SEQ), 1), 1.0, 0.0).astype(BF16)
    slot_of = named * (mm(named.astype(BF16), earlier) + 1.0)
    pos = iota((PEERS, PEERS), 0)
    named_at = jnp.zeros((PEERS, PEERS), jnp.int32)
    for p in range(PEERS):
        named_at = jnp.where(pos == p, peer_of(p, 1), named_at)
    order = jnp.where(named_at == iota((PEERS, PEERS), 1), 1.0, 0.0).astype(BF16)
    w_hi = weight.astype(BF16)
    w_lo = (weight - w_hi.astype(F32)).astype(BF16)
    slot_pt = mm(order, slot_of.astype(BF16)).astype(BF16)
    eye = jnp.where(iota((SEQ, SEQ), 0) == iota((SEQ, SEQ), 1), 1.0, 0.0).astype(BF16)

    def turned(v):
        return mm_nt(eye, v).astype(BF16)

    slot_tp = turned(slot_pt)
    whi_tp = turned(mm(order, w_hi).astype(BF16))
    wlo_tp = turned(mm(order, w_lo).astype(BF16))

    slot_p4 = jnp.concatenate([slot_pt] * QUARTERS, axis=1)
    row = iota((GROWS, QUARTERS * SEQ), 0)
    rowp = div_small(row, ROWS)
    rem_row = row - rowp * ROWS
    rowq = div_small(rem_row, SLOTS)
    rows_ = rem_row - rowq * SLOTS
    want = jnp.where(rowq == (iota((GROWS, QUARTERS * SEQ), 1) >> 6), rows_ + 1, -1).astype(F32)
    spread_row = div_small(iota((GROWS, PEERS), 0), ROWS)
    spread_col = iota((GROWS, PEERS), 1)
    for b in range(GROUPS):
        spread = jnp.where(spread_row + b * 8 == spread_col, 1.0, 0.0).astype(BF16)
        onehot[b * GROWS : (b + 1) * GROWS, :] = jnp.where(
            mm(spread, slot_p4) == want, 1.0, 0.0
        ).astype(BF16)

    loaded(out_gain, 10)
    loaded(out_proj, 11)
    loaded(ffn_gain, 12)
    act_copy.wait()
    a0 = actx[0].astype(F32)
    a1 = actx[1].astype(F32)
    mean_sq = (
        jnp.sum(a0 * a0, axis=1, keepdims=True) + jnp.sum(a1 * a1, axis=1, keepdims=True)
    ) * (1.0 / (2 * CHAN))
    scale = lax.rsqrt(mean_sq + EPS)
    s0 = (a0 * scale * out_gain[:, :CHAN]).astype(BF16)
    s1 = (a1 * scale * out_gain[:, CHAN:]).astype(BF16)
    after = (
        xv[tp].astype(F32) + (mm(s0, out_proj[:CHAN, :]) + mm(s1, out_proj[CHAN:, :]))
    ).astype(BF16)
    outv[...] = after
    after32 = after.astype(F32)
    sqx[tp] = jnp.broadcast_to(jnp.sum(after32 * after32, axis=1, keepdims=True), (SEQ, 128))
    sq_copy = to_partner(sqx.at[tp], local_sems.at[4], x_recv.at[1])
    sq_copy.start()

    def block_perm(rdim, cdim):
        r = iota((GROWS, GROWS), rdim)
        c = iota((GROWS, GROWS), cdim)
        rq = div_small(r, GSLOTS)
        rr = r - rq * GSLOTS
        rp = div_small(rr, SLOTS)
        rs = rr - rp * SLOTS
        return jnp.where(rp * ROWS + rq * SLOTS + rs == c, 1.0, 0.0).astype(BF16)

    perm[...] = block_perm(0, 1)
    permt[...] = block_perm(1, 0)

    col = iota((PEERS, ALL), 1)
    spread_t = jnp.where(div_small(col, ROWS) == iota((PEERS, ALL), 0), 1.0, 0.0).astype(BF16)
    c1 = iota((1, ALL), 1)
    c1 = c1 - div_small(c1, ROWS) * ROWS
    cq = div_small(c1, SLOTS)
    cs = (c1 - cq * SLOTS + 1).astype(F32)
    slot_x = mm(slot_tp, spread_t)
    whi_x = mm(whi_tp, spread_t)
    wlo_x = mm(wlo_tp, spread_t)
    hit = slot_x == cs
    for q in range(QUARTERS):
        keep = hit & (cq == q)
        chi[q * SEQ : (q + 1) * SEQ, :] = jnp.where(keep, whi_x, 0.0).astype(BF16)
        clo[q * SEQ : (q + 1) * SEQ, :] = jnp.where(keep, wlo_x, 0.0).astype(BF16)

    sq_copy.wait()
    mean_sq = (sqx[0] + sqx[1])[:, :1] * (1.0 / (2 * HALF))
    expert_in = (after32 * lax.rsqrt(mean_sq + EPS) * ffn_gain[tp]).astype(BF16)
    stacked = jnp.concatenate(
        [expert_in[:, q * QW : (q + 1) * QW] for q in range(QUARTERS)], axis=0
    )

    @pl.when(tp == 0)
    def _():
        pl.semaphore_wait(barrier, PEERS - 1)
        pl.semaphore_signal(hello, inc=1, device_id=(ep, other), device_id_type=MESH)

    @pl.when(tp == 1)
    def _():
        pl.semaphore_wait(hello, 1)

    def send_block(src, dst, p, sign, send, recv_):
        at = pl.ds(p * ROWS, ROWS)
        pltpu.make_async_remote_copy(
            src_ref=src.at[at], dst_ref=dst.at[at], send_sem=send, recv_sem=recv_,
            device_id=(peer_of(p, sign), tp), device_id_type=MESH,
        ).start()

    for b in range(4):
        rows = slice(b * 2 * GROWS, (b + 1) * 2 * GROWS)
        sendbuf[rows, :] = mm(onehot[rows, :], stacked).astype(BF16)
        for p in range(b * 2 * GP, min((b + 1) * 2 * GP, PEERS - 1)):
            send_block(sendbuf, recv.at[tp], p, 1, local_sems.at[7], d_recv.at[UNIT_OF[p // GP]])
    recv[tp, OWN:ALL, :] = sendbuf[OWN:ALL, :]

    loaded(wgu, 0)
    loaded(wd, 1)

    def arrived(ref, sem):
        pltpu.make_async_remote_copy(
            src_ref=ref, dst_ref=ref, send_sem=sem, recv_sem=sem,
            device_id=(ep, other), device_id_type=MESH,
        ).wait_recv()

    forwards = []

    def forward(u):
        first = UNITS[u][0] * GROWS
        last = (UNITS[u][-1] + 1) * GROWS
        arrived(recv.at[tp, pl.ds(first, min(last, OWN) - first)], d_recv.at[u])
        copy = to_partner(recv.at[tp, pl.ds(first, last - first)], local_sems.at[9], f_recv.at[u])
        copy.start()
        forwards.append(copy)

    def assemble(g):
        slots = slice(g * GSLOTS, (g + 1) * GSLOTS)
        for h in range(2):
            moved = mm(perm[...], recv[h, g * GROWS : (g + 1) * GROWS, :]).astype(BF16)
            for q in range(QUARTERS):
                amat[slots, h * HALF + q * QW : h * HALF + (q + 1) * QW] = moved[
                    q * GSLOTS : (q + 1) * GSLOTS, :
                ]

    forward(0)
    forward(1)
    for u in range(2):
        forwards[u].wait_recv()
        assemble(u)
    for c, chunk in enumerate(CHUNKS):
        following = CHUNKS[c + 1] if c + 1 < len(CHUNKS) else ()
        srows = slice(chunk[0] * GSLOTS, (chunk[-1] + 1) * GSLOTS)
        if c == 1:
            forward(3)
        lhs = amat[srows, :]
        for n in range(2):
            at = slice(n * 512, (n + 1) * 512)
            gate = mm(lhs, wgu[0, :, at])
            up = mm(lhs, wgu[1, :, at])
            gated = jnp.minimum(gate, LIMIT)
            act = (jnp.clip(up, -LIMIT, LIMIT) + 1.0) * gated * jax.nn.sigmoid(ALPHA * gated)
            hid[srows, at] = act.astype(BF16)
        if c == 0:
            forward(2)
        lhs = hid[srows, :]
        pieces = 1 if following else 2
        width = HALF // pieces
        parts = []
        for n in range(pieces):
            at = pl.ds(n * width, width)
            wat = pl.ds(pl.multiple_of(other * HALF + n * width, 512), width)
            psend[srows, at] = mm(lhs, wd[:, wat]).astype(BF16)
            part_copy = pltpu.make_async_remote_copy(
                src_ref=psend.at[srows, at], dst_ref=prec.at[srows, at],
                send_sem=local_sems.at[10], recv_sem=p_recv.at[c + n],
                device_id=(ep, other), device_id_type=MESH,
            )
            part_copy.start()
            parts.append(part_copy)
        if c == 1:
            forwards[3].wait_recv()
        wat = pl.ds(pl.multiple_of(tp * HALF, HALF), HALF)
        amat[srows, :HALF] = mm(lhs, wd[:, wat]).astype(BF16)
        if c == 0:
            forwards[2].wait_recv()
        for g in following:
            assemble(g)
        for part_copy in parts:
            part_copy.wait_recv()
        for g in chunk:
            slots = slice(g * GSLOTS, (g + 1) * GSLOTS)
            both = (amat[slots, :HALF].astype(F32) + prec[slots, :].astype(F32)).astype(BF16)
            tall = jnp.concatenate(
                [both[:, q * QW : (q + 1) * QW] for q in range(QUARTERS)], axis=0
            )
            rsend[g * GROWS : (g + 1) * GROWS, :] = mm(permt[...], tall).astype(BF16)
        for g in chunk:
            for p in range(g * GP, min((g + 1) * GP, PEERS - 1)):
                send_block(rsend, rrecv, p, -1, local_sems.at[8], r_recv.at[c])
    rrecv[OWN:ALL, :] = rsend[OWN:ALL, :]

    total = jnp.zeros((QUARTERS * SEQ, QW), F32)
    for c, chunk in enumerate(CHUNKS):
        first = chunk[0] * GROWS
        last = (chunk[-1] + 1) * GROWS
        arrived(rrecv.at[pl.ds(first, min(last, OWN) - first)], r_recv.at[c])
        got = rrecv[first:last, :]
        total = total + mm(chi[:, first:last], got) + mm(clo[:, first:last], got)
    for q in range(QUARTERS):
        cols = slice(q * QW, (q + 1) * QW)
        outv[:, cols] = (
            outv[:, cols].astype(F32) + total[q * SEQ : (q + 1) * SEQ, :]
        ).astype(BF16)
    store_out = pltpu.make_async_copy(outv, out_ref, local_sems.at[6])
    store_out.start()
    for sem, sent in (
        (7, sendbuf.at[pl.ds(0, OWN)]),
        (8, rsend.at[pl.ds(0, OWN)]),
        (9, recv.at[tp, pl.ds(0, ALL)]),
        (10, psend),
    ):
        pltpu.make_async_remote_copy(
            src_ref=sent, dst_ref=sent, send_sem=local_sems.at[sem], recv_sem=local_sems.at[sem],
            device_id=(ep, other), device_id_type=MESH,
        ).wait_send()
    store_state.wait()
    store_out.wait()


def store(u_in, s_in, u_out, s_out, u_buf, s_buf, in_sems, out_sems):
    pieces = [
        (s_in.at[i, pl.ds(r, 32)], s_buf.at[i, pl.ds(r, 32)], s_out.at[i, pl.ds(r, 32)])
        for i in range(2)
        for r in range(0, SEQ, 32)
    ]
    pieces.append((u_in, u_buf, u_out))
    loads = [pltpu.make_async_copy(a, b, in_sems.at[i]) for i, (a, b, _) in enumerate(pieces)]
    stores = [pltpu.make_async_copy(b, c, out_sems.at[i]) for i, (_, b, c) in enumerate(pieces)]
    for load in loads:
        load.start()
    for load, put in zip(loads, stores):
        load.wait()
        put.start()
    for put in stores:
        put.wait()


def local(
    residual,
    route_ids,
    route_weights,
    carried_state,
    mix_gain,
    in_proj,
    decay_rate,
    frequency,
    step_size,
    input_map,
    output_matrix,
    passthrough_scale,
    out_gain,
    out_proj,
    ffn_gain,
    w_gate,
    w_up,
    w_down,
):
    ids, wts = route_ids.T, route_weights.T
    maps = (
        jnp.swapaxes(input_map, 2, 3).reshape(2, CHAN, -1),
        output_matrix.reshape(2, CHAN, -1),
    )
    args = (
        residual,
        ids,
        wts,
        decay_rate,
        frequency,
        step_size.reshape(1, -1),
        *maps,
        mix_gain.reshape(1, -1),
        in_proj,
        carried_state,
        passthrough_scale.reshape(1, -1),
        out_gain.reshape(1, -1),
        out_proj,
        ffn_gain.reshape(2, 1, -1),
        w_gate.reshape(w_gate.shape[1:]),
        w_up.reshape(w_up.shape[1:]),
        w_down.reshape(w_down.shape[1:]),
    )
    dma = pltpu.SemaphoreType.DMA
    vmem = pltpu.VMEM
    out_shape = (
        jax.ShapeDtypeStruct(residual.shape, BF16),
        jax.ShapeDtypeStruct(carried_state.shape, F32),
    )
    results = pl.pallas_call(
        kernel,
        out_shape=out_shape,
        in_specs=[pl.BlockSpec(memory_space=pl.ANY)] * len(args),
        out_specs=(pl.BlockSpec(memory_space=pl.ANY),) * 2,
        scratch_shapes=[
            vmem(residual.shape, BF16),
            vmem(carried_state.shape, F32),
            vmem((2, *residual.shape), BF16),
        ]
        + [vmem(a.shape, a.dtype) for a in (ids, wts)]
        + [
            vmem((2, *decay_rate.shape), F32),
            vmem((1, step_size.shape[0]), F32),
            vmem((2, *maps[0].shape), F32),
            vmem((1, mix_gain.shape[0]), F32),
            vmem(in_proj.shape, BF16),
            vmem(carried_state.shape, F32),
            vmem((1, CHAN), F32),
            vmem((1, 2 * CHAN), F32),
            vmem(out_proj.shape, BF16),
            vmem((2, 1, HALF), F32),
            vmem((2, *w_gate.shape[1:]), BF16),
            vmem(w_down.shape[1:], BF16),
            vmem((2, CHAN, 512), BF16),
            vmem((2, CHAN, 512), BF16),
            vmem((2, SEQ, CHAN), BF16),
            vmem((2, SEQ, 128), F32),
            vmem((ALL, QUARTERS * SEQ), BF16),
            vmem((QUARTERS * SEQ, ALL), BF16),
            vmem((QUARTERS * SEQ, ALL), BF16),
            vmem((GROWS, GROWS), BF16),
            vmem((GROWS, GROWS), BF16),
            vmem((PAD, QW), BF16),
            vmem((2, PAD, QW), BF16),
            vmem((PAD, QW), BF16),
            vmem((PAD, QW), BF16),
            vmem((PEERS * SLOTS, 2 * HALF), BF16),
            vmem((PEERS * SLOTS, HALF), BF16),
            vmem((PEERS * SLOTS, HALF), BF16),
            vmem((PEERS * SLOTS, HALF), BF16),
            dma((13,)),
            pltpu.SemaphoreType.REGULAR,
            dma((3,)),
            dma((len(UNITS),)),
            dma((len(UNITS),)),
            dma((len(CHUNKS) + 1,)),
            dma((len(CHUNKS),)),
        ],
        compiler_params=pltpu.CompilerParams(
            collective_id=0, has_side_effects=True, vmem_limit_bytes=VMEM_LIMIT
        ),
    )(*args)
    return pl.pallas_call(
        store,
        out_shape=out_shape,
        in_specs=[pl.BlockSpec(memory_space=pl.ANY)] * 2,
        out_specs=(pl.BlockSpec(memory_space=pl.ANY),) * 2,
        scratch_shapes=[
            vmem(residual.shape, BF16),
            vmem(carried_state.shape, F32),
            dma((5,)),
            dma((5,)),
        ],
        compiler_params=pltpu.CompilerParams(vmem_limit_bytes=VMEM_LIMIT),
    )(*results)


def solution(mesh):
    placed = (
        P("ep", "tp"),
        P("ep", None),
        P("ep", None),
        P(None, "ep", "tp"),
        P(),
        P(None, "tp"),
        P("tp", None),
        P("tp", None),
        P("tp"),
        P(None, "tp", None, None),
        P(None, "tp", None, None),
        P("tp"),
        P(),
        P(None, "tp"),
        P(),
        P("ep", None, "tp"),
        P("ep", None, "tp"),
        P("ep", "tp", None),
    )
    return jax.shard_map(
        local,
        mesh=mesh,
        in_specs=placed,
        out_specs=(P("ep", "tp"), P(None, "ep", "tp")),
        check_vma=False,
    )
```

```python
import jax
import jax.numpy as jnp
from jax import lax
from jax.experimental import pallas as pl
from jax.experimental.pallas import tpu as pltpu
from jax.sharding import PartitionSpec as P

F32 = jnp.float32
BF16 = jnp.bfloat16
MESH = pl.DeviceIdType.MESH

AHEAD = 2
VMEM_LIMIT = 62 * 1024 * 1024
EPS = 1e-06
LIMIT = 7.0
ALPHA = 1.702

SEQ = 64
HALF = 1024
STATES = 2048
CHAN = 512
PEERS = 64
SLOTS = 6
QUARTERS = 4
QW = HALF // QUARTERS
ROWS = SLOTS * QUARTERS
ALL = PEERS * ROWS
PAD = ALL + 8
OWN = ALL - ROWS
GROUPS = 8
GP = PEERS // GROUPS
GROWS = GP * ROWS
GSLOTS = GP * SLOTS
CHUNKS = ((0, 1), (2, 3, 4), (5, 6, 7))
UNITS = ((0,), (1,), (2, 3, 4), (5, 6, 7))

UNIT_OF = {g: u for u, unit in enumerate(UNITS) for g in unit}


def hops(step):
    return sum(min(d, 4 - d) for d in step)


STEPS = sorted(
    ((dz, dy, dx) for dz in range(4) for dy in range(4) for dx in range(4)), key=hops, reverse=True
)

NT = (((1,), (1,)), ((), ()))


def mm(a, b):
    return jnp.dot(a, b, preferred_element_type=F32)


def mm_nt(a, b):
    return lax.dot_general(a, b, NT, preferred_element_type=F32)


def iota(shape, dim):
    return lax.broadcasted_iota(jnp.int32, shape, dim)


def div_small(v, d):
    return ((v.astype(F32) + 0.5) * (1.0 / d)).astype(jnp.int32)


def kernel(
    x_in,
    ids_in,
    wts_in,
    decay_in,
    freq_in,
    step_in,
    imap_in,
    omap_in,
    mix_gain_in,
    in_proj_in,
    state_in,
    pscale_in,
    out_gain_in,
    out_proj_in,
    ffn_gain_in,
    wg_in,
    wu_in,
    wd_in,
    out_ref,
    nstate_ref,
    outv,
    nstate,
    xv,
    ids,
    wts,
    rates,
    step,
    maps,
    mix_gain,
    in_proj,
    state,
    pscale,
    out_gain,
    out_proj,
    ffn_gain,
    wgu,
    wd,
    inmix,
    outmix,
    actx,
    sqx,
    onehot,
    chi,
    perm,
    permt,
    sendbuf,
    recv,
    rsend,
    rrecv,
    amat,
    hid,
    own,
    psend,
    prec,
    local_sems,
    hello,
    x_recv,
    d_recv,
    f_recv,
    p_recv,
    r_recv,
):
    ep = lax.axis_index("ep")
    tp = lax.axis_index("tp")
    other = 1 - tp
    z = lax.div(ep, 16)
    y = lax.rem(lax.div(ep, 4), 4)
    x = lax.rem(ep, 4)
    z_at = [lax.rem(z + d, 4) * 16 for d in range(4)]
    y_at = [lax.rem(y + d, 4) * 4 for d in range(4)]
    x_at = [lax.rem(x + d, 4) for d in range(4)]

    def peer_of(p, sign):
        dz, dy, dx = STEPS[p]
        return z_at[sign * dz % 4] + y_at[sign * dy % 4] + x_at[sign * dx % 4]

    pairs = (
        (x_in, xv.at[tp], 0),
        (in_proj_in, in_proj, 5),
        (decay_in, rates.at[0], 1),
        (freq_in, rates.at[1], 1),
        (step_in, step, 2),
        (imap_in, maps.at[0], 3),
        (omap_in, maps.at[1], 3),
        (mix_gain_in, mix_gain, 6),
        (state_in, state, 4),
        (pscale_in, pscale, 7),
        (ids_in, ids, 8),
        (wts_in, wts, 9),
        (out_gain_in, out_gain, 10),
        (ffn_gain_in, ffn_gain, 12),
        (out_proj_in, out_proj, 11),
        (wg_in, wgu.at[0], 0),
        (wu_in, wgu.at[1], 0),
        (wd_in, wd, 1),
    )

    def loaded(ref, sem):
        pltpu.make_async_copy(ref, ref, local_sems.at[sem]).wait()

    loads = [pltpu.make_async_copy(a, b, local_sems.at[i]) for a, b, i in pairs]
    loads[0].start()
    barrier = pltpu.get_barrier_semaphore()

    @pl.when(tp == 0)
    def _():
        pl.semaphore_signal(barrier, inc=1, device_id=(ep, other), device_id_type=MESH)

    for load in loads[1:14]:
        load.start()

    @pl.when(tp == 1)
    def _():
        pl.semaphore_wait(barrier, 1)
        pl.semaphore_signal(hello, inc=1, device_id=(ep, other), device_id_type=MESH)

    @pl.when(tp == 0)
    def _():
        pl.semaphore_wait(hello, 1)

        def greet(i, carry):
            pl.semaphore_signal(
                barrier, inc=1, device_id=(lax.rem(ep + i, PEERS), tp), device_id_type=MESH
            )
            return carry

        lax.fori_loop(1, PEERS, greet, 0)


    loaded(xv.at[tp], 0)

    def to_partner(ref, send, recv_):
        return pltpu.make_async_remote_copy(
            src_ref=ref, dst_ref=ref, send_sem=send, recv_sem=recv_,
            device_id=(ep, other), device_id_type=MESH,
        )

    x_copy = to_partner(xv.at[tp], local_sems.at[0], x_recv.at[2])
    x_copy.start()

    loaded(rates, 1)
    loaded(step, 2)
    rate_real = -rates[0]
    rate_imag = rates[1]
    n_groups, n_state = rate_real.shape
    diag = iota((n_groups, n_groups), 0) == iota((n_groups, n_groups), 1)
    time_step = jnp.sum(jnp.where(diag, step[...], 0.0), axis=1, keepdims=True)
    magnitude = jnp.exp(rate_real * time_step)
    phase = rate_imag * time_step
    bar_real = magnitude * jnp.cos(phase)
    bar_imag = magnitude * jnp.sin(phase)
    denominator = rate_real * rate_real + rate_imag * rate_imag
    shifted = bar_real - 1.0
    coef_real = (shifted * rate_real + bar_imag * rate_imag) / denominator
    coef_imag = (bar_imag * rate_real - shifted * rate_imag) / denominator
    own_group = iota((n_groups, STATES), 0) == (iota((n_groups, STATES), 1) >> 6)

    def as_row(v):
        wide = jnp.concatenate([v] * (STATES // n_state), axis=1)
        return jnp.sum(jnp.where(own_group, wide, 0.0), axis=0, keepdims=True)

    bar_real, bar_imag, coef_real, coef_imag = (
        as_row(v) for v in (bar_real, bar_imag, coef_real, coef_imag)
    )

    same = (iota((128, 512), 0) >> 4) == (iota((128, 512), 1) >> 6)

    def spread_groups(m):
        return jnp.where(same, jnp.concatenate([m] * 8, axis=1), 0.0).astype(BF16)

    loaded(maps, 3)
    for b in range(4):
        rows = slice(b * 128, (b + 1) * 128)
        for i in range(2):
            inmix[i, rows, :] = spread_groups(maps[0, i, rows, :])
        outmix[0, rows, :] = spread_groups(maps[1, 0, rows, :])
        outmix[1, rows, :] = spread_groups(-maps[1, 1, rows, :])

    loaded(state, 4)
    for b in range(4):
        cols = slice(b * 512, (b + 1) * 512)
        hr = state[0, :, cols]
        hi = state[1, :, cols]
        br, bi = bar_real[:, cols], bar_imag[:, cols]
        nstate[0, :, cols] = br * hr - bi * hi
        nstate[1, :, cols] = br * hi + bi * hr
    loaded(in_proj, 5)
    loaded(mix_gain, 6)
    loaded(pscale, 7)
    x_copy.wait()
    x0 = xv[0].astype(F32)
    x1 = xv[1].astype(F32)
    mean_sq = (
        jnp.sum(x0 * x0, axis=1, keepdims=True) + jnp.sum(x1 * x1, axis=1, keepdims=True)
    ) * (1.0 / (2 * HALF))
    scale = lax.rsqrt(mean_sq + EPS)
    n0 = (x0 * scale * mix_gain[:, :HALF]).astype(BF16)
    n1 = (x1 * scale * mix_gain[:, HALF:]).astype(BF16)
    for load in loads[14:]:
        load.start()
    channels = (mm(n0, in_proj[:HALF, :]) + mm(n1, in_proj[HALF:, :])).astype(BF16)
    spans = [(slice(b * 128, (b + 1) * 128), slice(b * 512, (b + 1) * 512)) for b in range(4)]
    pushes = [
        (mm(channels[:, rows], inmix[0, rows, :]), mm(channels[:, rows], inmix[1, rows, :]))
        for rows, _ in spans
    ]
    states = []
    for (rows, cols), (u0, u1) in zip(spans, pushes):
        cr, ci = coef_real[:, cols], coef_imag[:, cols]
        nr = nstate[0, :, cols] + (cr * u0 - ci * u1)
        ni = nstate[1, :, cols] + (cr * u1 + ci * u0)
        nstate[0, :, cols] = nr
        nstate[1, :, cols] = ni
        states.append((nr.astype(BF16), ni.astype(BF16)))
    mixed = jnp.concatenate(
        [
            mm_nt(nr, outmix[0, rows, :]) + mm_nt(ni, outmix[1, rows, :])
            for (rows, _), (nr, ni) in zip(spans, states)
        ],
        axis=1,
    ) + pscale[...] * channels.astype(F32)
    actx[tp] = jax.nn.gelu(mixed, approximate=True).astype(BF16)

    store_state = pltpu.make_async_copy(nstate, nstate_ref, local_sems.at[5])
    store_state.start()
    act_copy = to_partner(actx.at[tp], local_sems.at[3], x_recv.at[0])
    act_copy.start()

    loaded(ids, 8)
    loaded(wts, 9)
    expert = iota((PEERS, SEQ), 0)
    named = jnp.zeros((PEERS, SEQ), F32)
    weight = jnp.zeros((PEERS, SEQ), F32)
    for k in range(4):
        hit = ids[k : k + 1, :] == expert
        named = named + jnp.where(hit, 1.0, 0.0)
        weight = weight + jnp.where(hit, wts[k : k + 1, :], 0.0)
    earlier = jnp.where(iota((SEQ, SEQ), 0) < iota((SEQ, SEQ), 1), 1.0, 0.0).astype(BF16)
    slot_of = named * (mm(named.astype(BF16), earlier) + 1.0)
    pos = iota((PEERS, PEERS), 0)
    named_at = jnp.zeros((PEERS, PEERS), jnp.int32)
    for p in range(PEERS):
        named_at = jnp.where(pos == p, peer_of(p, 1), named_at)
    order = jnp.where(named_at == iota((PEERS, PEERS), 1), 1.0, 0.0).astype(BF16)
    w_hi = weight.astype(BF16)
    slot_pt = mm(order, slot_of.astype(BF16)).astype(BF16)
    eye = jnp.where(iota((SEQ, SEQ), 0) == iota((SEQ, SEQ), 1), 1.0, 0.0).astype(BF16)

    def turned(v):
        return mm_nt(eye, v).astype(BF16)

    slot_tp = turned(slot_pt)
    whi_tp = turned(mm(order, w_hi).astype(BF16))

    slot_p4 = jnp.concatenate([slot_pt] * QUARTERS, axis=1)
    row = iota((GROWS, QUARTERS * SEQ), 0)
    rowp = div_small(row, ROWS)
    rem_row = row - rowp * ROWS
    rowq = div_small(rem_row, SLOTS)
    rows_ = rem_row - rowq * SLOTS
    want = jnp.where(rowq == (iota((GROWS, QUARTERS * SEQ), 1) >> 6), rows_ + 1, -1).astype(F32)
    spread_row = div_small(iota((GROWS, PEERS), 0), ROWS)
    spread_col = iota((GROWS, PEERS), 1)
    for b in range(GROUPS):
        spread = jnp.where(spread_row + b * 8 == spread_col, 1.0, 0.0).astype(BF16)
        onehot[b * GROWS : (b + 1) * GROWS, :] = jnp.where(
            mm(spread, slot_p4) == want, 1.0, 0.0
        ).astype(BF16)

    loaded(out_gain, 10)
    loaded(out_proj, 11)
    loaded(ffn_gain, 12)
    act_copy.wait()
    a0 = actx[0].astype(F32)
    a1 = actx[1].astype(F32)
    mean_sq = (
        jnp.sum(a0 * a0, axis=1, keepdims=True) + jnp.sum(a1 * a1, axis=1, keepdims=True)
    ) * (1.0 / (2 * CHAN))
    scale = lax.rsqrt(mean_sq + EPS)
    s0 = (a0 * scale * out_gain[:, :CHAN]).astype(BF16)
    s1 = (a1 * scale * out_gain[:, CHAN:]).astype(BF16)
    after = (
        xv[tp].astype(F32) + (mm(s0, out_proj[:CHAN, :]) + mm(s1, out_proj[CHAN:, :]))
    ).astype(BF16)
    outv[...] = after
    after32 = after.astype(F32)
    sqx[tp] = jnp.broadcast_to(jnp.sum(after32 * after32, axis=1, keepdims=True), (SEQ, 128))
    sq_copy = to_partner(sqx.at[tp], local_sems.at[4], x_recv.at[1])
    sq_copy.start()

    @pl.when(tp == 0)
    def _():
        pl.semaphore_wait(barrier, PEERS - 1)
        pl.semaphore_signal(hello, inc=1, device_id=(ep, other), device_id_type=MESH)

    def send_block(src, dst, p, sign, send, recv_):
        at = pl.ds(p * ROWS, ROWS)
        pltpu.make_async_remote_copy(
            src_ref=src.at[at], dst_ref=dst.at[at], send_sem=send, recv_sem=recv_,
            device_id=(peer_of(p, sign), tp), device_id_type=MESH,
        ).start()

    def gather(b, values):
        stacked = jnp.concatenate(
            [values[:, q * QW : (q + 1) * QW] for q in range(QUARTERS)], axis=0
        )
        rows = slice(b[0] * GROWS, (b[-1] + 1) * GROWS)
        sendbuf[rows, :] = mm(onehot[rows, :], stacked).astype(BF16)

    def dispatch(b):
        for p in range(b[0] * GP, min((b[-1] + 1) * GP, PEERS - 1)):
            send_block(sendbuf, recv.at[tp], p, 1, local_sems.at[7], d_recv.at[UNIT_OF[p // GP]])


    gather(CHUNKS[0], after)

    @pl.when(tp == 1)
    def _():
        pl.semaphore_wait(hello, 1)

    dispatch(CHUNKS[0])

    def block_perm(rdim, cdim):
        r = iota((GROWS, GROWS), rdim)
        c = iota((GROWS, GROWS), cdim)
        rq = div_small(r, GSLOTS)
        rr = r - rq * GSLOTS
        rp = div_small(rr, SLOTS)
        rs = rr - rp * SLOTS
        return jnp.where(rp * ROWS + rq * SLOTS + rs == c, 1.0, 0.0).astype(BF16)

    perm[...] = block_perm(0, 1)
    permt[...] = block_perm(1, 0)

    sq_copy.wait()
    mean_sq = (sqx[0] + sqx[1])[:, :1] * (1.0 / (2 * HALF))
    expert_in = (after32 * lax.rsqrt(mean_sq + EPS) * ffn_gain[tp]).astype(BF16)
    for b in CHUNKS[1:]:
        gather(b, expert_in)
        dispatch(b)
    recv[tp, OWN:ALL, :] = sendbuf[OWN:ALL, :]

    col = iota((PEERS, ALL), 1)
    spread_t = jnp.where(div_small(col, ROWS) == iota((PEERS, ALL), 0), 1.0, 0.0).astype(BF16)
    c1 = iota((1, ALL), 1)
    c1 = c1 - div_small(c1, ROWS) * ROWS
    cq = div_small(c1, SLOTS)
    cs = (c1 - cq * SLOTS + 1).astype(F32)
    slot_x = mm(slot_tp, spread_t)
    whi_x = mm(whi_tp, spread_t)
    hit = slot_x == cs
    for q in range(QUARTERS):
        keep = hit & (cq == q)
        chi[q * SEQ : (q + 1) * SEQ, :] = jnp.where(keep, whi_x, 0.0).astype(BF16)

    loaded(wgu, 0)
    loaded(wd, 1)

    def arrived(ref, sem):
        pltpu.make_async_remote_copy(
            src_ref=ref, dst_ref=ref, send_sem=sem, recv_sem=sem,
            device_id=(ep, other), device_id_type=MESH,
        ).wait_recv()

    def passed_on(u):
        first = UNITS[u][0] * GROWS
        last = (UNITS[u][-1] + 1) * GROWS
        return first, last, to_partner(
            recv.at[tp, pl.ds(first, last - first)], local_sems.at[9], f_recv.at[u]
        )

    def forward(u):
        first, last, copy = passed_on(u)
        arrived(recv.at[tp, pl.ds(first, min(last, OWN) - first)], d_recv.at[u])
        copy.start()

    def assemble(g):
        slots = slice(g * GSLOTS, (g + 1) * GSLOTS)
        moved = [mm(perm[...], recv[h, g * GROWS : (g + 1) * GROWS, :]) for h in range(2)]
        pieces = [
            (h, slice(q * QW, (q + 1) * QW), moved[h][q * GSLOTS : (q + 1) * GSLOTS, :])
            for h in range(2)
            for q in range(QUARTERS)
        ]
        if g in CHUNKS[0]:
            squares = pieces[0][2] * pieces[0][2]
            for _, _, piece in pieces[1:]:
                squares = squares + piece * piece
            mean_sq = jnp.sum(squares, axis=1, keepdims=True) * (1.0 / (2 * HALF))
            scale = lax.rsqrt(mean_sq + EPS)
            pieces = [(h, at, piece * scale * ffn_gain[h, :, at]) for h, at, piece in pieces]
        for h, at, piece in pieces:
            amat[slots, h * HALF + at.start : h * HALF + at.stop] = piece.astype(BF16)

    def experts(order):
        units_of = [[u for u in range(len(UNITS)) if UNITS[u][0] in CHUNKS[c]] for c in order] + [[]]
        for u in units_of[0]:
            forward(u)
        for u in units_of[0]:
            passed_on(u)[2].wait_recv()
            for g in UNITS[u]:
                assemble(g)

        def units(c, halves):
            srows = slice(CHUNKS[c][0] * GSLOTS, (CHUNKS[c][-1] + 1) * GSLOTS)
            lhs = amat[srows, :]
            for n in halves:
                at = slice(n * 512, (n + 1) * 512)
                gate = mm(lhs, wgu[0, :, at])
                up = mm(lhs, wgu[1, :, at])
                gated = jnp.minimum(gate, LIMIT)
                act = (jnp.clip(up, -LIMIT, LIMIT) + 1.0) * gated * jax.nn.sigmoid(ALPHA * gated)
                hid[srows, at] = act.astype(BF16)

        for i, c in enumerate(order):
            chunk = CHUNKS[c]
            last = i + 1 == len(order)
            srows = slice(chunk[0] * GSLOTS, (chunk[-1] + 1) * GSLOTS)
            if i == 1:
                for u in units_of[i + 1]:
                    forward(u)
            units(c, (1,) if i >= AHEAD else (0, 1))
            if i == 0:
                for u in units_of[i + 1]:
                    forward(u)
            lhs = hid[srows, :]
            pieces = 2 if last else 1
            width = HALF // pieces
            parts = []
            for n in range(pieces):
                at = pl.ds(n * width, width)
                wat = pl.ds(pl.multiple_of(other * HALF + n * width, 512), width)
                psend[srows, at] = mm(lhs, wd[:, wat]).astype(BF16)
                part_copy = pltpu.make_async_remote_copy(
                    src_ref=psend.at[srows, at], dst_ref=prec.at[srows, at],
                    send_sem=local_sems.at[10], recv_sem=p_recv.at[i + n],
                    device_id=(ep, other), device_id_type=MESH,
                )
                part_copy.start()
                parts.append(part_copy)
            if i == 1:
                for u in units_of[i + 1]:
                    passed_on(u)[2].wait_recv()
            own[srows, :] = mm(lhs, wd[:, pl.ds(pl.multiple_of(tp * HALF, HALF), HALF)]).astype(BF16)
            if i == 0:
                for u in units_of[i + 1]:
                    passed_on(u)[2].wait_recv()
            for u in units_of[i + 1]:
                for g in UNITS[u]:
                    assemble(g)
            if not last and i + 1 >= AHEAD:
                units(order[i + 1], (0,))
            for part_copy in parts:
                part_copy.wait_recv()
            for g in chunk:
                slots = slice(g * GSLOTS, (g + 1) * GSLOTS)
                both = (own[slots, :].astype(F32) + prec[slots, :].astype(F32)).astype(BF16)
                tall = jnp.concatenate(
                    [both[:, q * QW : (q + 1) * QW] for q in range(QUARTERS)], axis=0
                )
                rsend[g * GROWS : (g + 1) * GROWS, :] = mm(permt[...], tall).astype(BF16)
            for g in chunk:
                for p in range(g * GP, min((g + 1) * GP, PEERS - 1)):
                    send_block(rsend, rrecv, p, -1, local_sems.at[8], r_recv.at[c])

    experts(tuple(range(len(CHUNKS))))
    rrecv[OWN:ALL, :] = rsend[OWN:ALL, :]

    total = jnp.zeros((QUARTERS * SEQ, QW), F32)
    for c, chunk in enumerate(CHUNKS):
        first = chunk[0] * GROWS
        last = (chunk[-1] + 1) * GROWS
        arrived(rrecv.at[pl.ds(first, min(last, OWN) - first)], r_recv.at[c])
        got = rrecv[first:last, :]
        total = total + mm(chi[:, first:last], got)
    for q in range(QUARTERS):
        cols = slice(q * QW, (q + 1) * QW)
        outv[:, cols] = (
            outv[:, cols].astype(F32) + total[q * SEQ : (q + 1) * SEQ, :]
        ).astype(BF16)
    store_out = pltpu.make_async_copy(outv, out_ref, local_sems.at[6])
    store_out.start()
    for sem, sent in (
        (7, sendbuf.at[pl.ds(0, OWN)]),
        (8, rsend.at[pl.ds(0, OWN)]),
        (9, recv.at[tp, pl.ds(0, ALL)]),
        (10, psend),
    ):
        pltpu.make_async_remote_copy(
            src_ref=sent, dst_ref=sent, send_sem=local_sems.at[sem], recv_sem=local_sems.at[sem],
            device_id=(ep, other), device_id_type=MESH,
        ).wait_send()
    store_state.wait()
    store_out.wait()


def store(u_in, s_in, u_out, s_out, u_buf, s_buf, in_sems, out_sems):
    pieces = [
        (s_in.at[i, pl.ds(r, 32)], s_buf.at[i, pl.ds(r, 32)], s_out.at[i, pl.ds(r, 32)])
        for i in range(2)
        for r in range(0, SEQ, 32)
    ]
    pieces.append((u_in, u_buf, u_out))
    loads = [pltpu.make_async_copy(a, b, in_sems.at[i]) for i, (a, b, _) in enumerate(pieces)]
    stores = [pltpu.make_async_copy(b, c, out_sems.at[i]) for i, (_, b, c) in enumerate(pieces)]
    for load in loads:
        load.start()
    for load, put in zip(loads, stores):
        load.wait()
        put.start()
    for put in stores:
        put.wait()


def local(
    residual,
    route_ids,
    route_weights,
    carried_state,
    mix_gain,
    in_proj,
    decay_rate,
    frequency,
    step_size,
    input_map,
    output_matrix,
    passthrough_scale,
    out_gain,
    out_proj,
    ffn_gain,
    w_gate,
    w_up,
    w_down,
):
    ids, wts = route_ids.T, route_weights.T
    maps = (
        jnp.swapaxes(input_map, 2, 3).reshape(2, CHAN, -1),
        output_matrix.reshape(2, CHAN, -1),
    )
    args = (
        residual,
        ids,
        wts,
        decay_rate,
        frequency,
        step_size.reshape(1, -1),
        *maps,
        mix_gain.reshape(1, -1),
        in_proj,
        carried_state,
        passthrough_scale.reshape(1, -1),
        out_gain.reshape(1, -1),
        out_proj,
        ffn_gain.reshape(2, 1, -1),
        w_gate.reshape(w_gate.shape[1:]),
        w_up.reshape(w_up.shape[1:]),
        w_down.reshape(w_down.shape[1:]),
    )
    dma = pltpu.SemaphoreType.DMA
    vmem = pltpu.VMEM
    out_shape = (
        jax.ShapeDtypeStruct(residual.shape, BF16),
        jax.ShapeDtypeStruct(carried_state.shape, F32),
    )
    results = pl.pallas_call(
        kernel,
        out_shape=out_shape,
        in_specs=[pl.BlockSpec(memory_space=pl.ANY)] * len(args),
        out_specs=(pl.BlockSpec(memory_space=pl.ANY),) * 2,
        scratch_shapes=[
            vmem(residual.shape, BF16),
            vmem(carried_state.shape, F32),
            vmem((2, *residual.shape), BF16),
        ]
        + [vmem(a.shape, a.dtype) for a in (ids, wts)]
        + [
            vmem((2, *decay_rate.shape), F32),
            vmem((1, step_size.shape[0]), F32),
            vmem((2, *maps[0].shape), F32),
            vmem((1, mix_gain.shape[0]), F32),
            vmem(in_proj.shape, BF16),
            vmem(carried_state.shape, F32),
            vmem((1, CHAN), F32),
            vmem((1, 2 * CHAN), F32),
            vmem(out_proj.shape, BF16),
            vmem((2, 1, HALF), F32),
            vmem((2, *w_gate.shape[1:]), BF16),
            vmem(w_down.shape[1:], BF16),
            vmem((2, CHAN, 512), BF16),
            vmem((2, CHAN, 512), BF16),
            vmem((2, SEQ, CHAN), BF16),
            vmem((2, SEQ, 128), F32),
            vmem((ALL, QUARTERS * SEQ), BF16),
            vmem((QUARTERS * SEQ, ALL), BF16),
            vmem((GROWS, GROWS), BF16),
            vmem((GROWS, GROWS), BF16),
            vmem((PAD, QW), BF16),
            vmem((2, PAD, QW), BF16),
            vmem((PAD, QW), BF16),
            vmem((PAD, QW), BF16),
            vmem((PEERS * SLOTS, 2 * HALF), BF16),
            vmem((PEERS * SLOTS, HALF), BF16),
            vmem((PEERS * SLOTS, HALF), BF16),
            vmem((PEERS * SLOTS, HALF), BF16),
            vmem((PEERS * SLOTS, HALF), BF16),
            dma((13,)),
            pltpu.SemaphoreType.REGULAR,
            dma((3,)),
            dma((len(UNITS),)),
            dma((len(UNITS),)),
            dma((len(CHUNKS) + 1,)),
            dma((len(CHUNKS),)),
        ],
        compiler_params=pltpu.CompilerParams(
            collective_id=0, has_side_effects=True, vmem_limit_bytes=VMEM_LIMIT
        ),
    )(*args)
    return pl.pallas_call(
        store,
        out_shape=out_shape,
        in_specs=[pl.BlockSpec(memory_space=pl.ANY)] * 2,
        out_specs=(pl.BlockSpec(memory_space=pl.ANY),) * 2,
        scratch_shapes=[
            vmem(residual.shape, BF16),
            vmem(carried_state.shape, F32),
            dma((5,)),
            dma((5,)),
        ],
        compiler_params=pltpu.CompilerParams(vmem_limit_bytes=VMEM_LIMIT),
    )(*results)


def solution(mesh):
    placed = (
        P("ep", "tp"),
        P("ep", None),
        P("ep", None),
        P(None, "ep", "tp"),
        P(),
        P(None, "tp"),
        P("tp", None),
        P("tp", None),
        P("tp"),
        P(None, "tp", None, None),
        P(None, "tp", None, None),
        P("tp"),
        P(),
        P(None, "tp"),
        P(),
        P("ep", None, "tp"),
        P("ep", None, "tp"),
        P("ep", "tp", None),
    )
    return jax.shard_map(
        local,
        mesh=mesh,
        in_specs=placed,
        out_specs=(P("ep", "tp"), P(None, "ep", "tp")),
        check_vma=False,
    )
```

```python
import jax
import jax.numpy as jnp
from jax import lax
from jax.experimental import pallas as pl
from jax.experimental.pallas import tpu as pltpu
from jax.sharding import PartitionSpec as P

F32 = jnp.float32
BF16 = jnp.bfloat16
MESH = pl.DeviceIdType.MESH

AHEAD = 2
VMEM_LIMIT = 62 * 1024 * 1024
EPS = 1e-06
LIMIT = 7.0
ALPHA = 1.702

SEQ = 64
HALF = 1024
STATES = 2048
CHAN = 512
PEERS = 64
SLOTS = 6
QUARTERS = 4
QW = HALF // QUARTERS
ROWS = SLOTS * QUARTERS
ALL = PEERS * ROWS
PAD = ALL + 8
OWN = ALL - ROWS
GROUPS = 8
GP = PEERS // GROUPS
GROWS = GP * ROWS
GSLOTS = GP * SLOTS
CHUNKS = ((0, 1), (2, 3, 4), (5, 6, 7))
UNITS = ((0,), (1,), (2, 3, 4), (5, 6, 7))

UNIT_OF = {g: u for u, unit in enumerate(UNITS) for g in unit}


def hops(step):
    return sum(min(d, 4 - d) for d in step)


STEPS = sorted(
    ((dz, dy, dx) for dz in range(4) for dy in range(4) for dx in range(4)), key=hops, reverse=True
)

NT = (((1,), (1,)), ((), ()))


def mm(a, b):
    return jnp.dot(a, b, preferred_element_type=F32)


def mm_nt(a, b):
    return lax.dot_general(a, b, NT, preferred_element_type=F32)


def iota(shape, dim):
    return lax.broadcasted_iota(jnp.int32, shape, dim)


def div_small(v, d):
    return ((v.astype(F32) + 0.5) * (1.0 / d)).astype(jnp.int32)


def kernel(
    x_in,
    ids_in,
    wts_in,
    decay_in,
    freq_in,
    step_in,
    imap_in,
    omap_in,
    mix_gain_in,
    in_proj_in,
    state_in,
    pscale_in,
    out_gain_in,
    out_proj_in,
    ffn_gain_in,
    wg_in,
    wu_in,
    wd_in,
    out_ref,
    nstate_ref,
    outv,
    nstate,
    xv,
    ids,
    wts,
    rates,
    step,
    maps,
    mix_gain,
    in_proj,
    state,
    pscale,
    out_gain,
    out_proj,
    ffn_gain,
    wgu,
    wd,
    inmix,
    outmix,
    actx,
    sqx,
    onehot,
    chi,
    perm,
    permt,
    sendbuf,
    recv,
    rsend,
    rrecv,
    amat,
    hid,
    own,
    psend,
    prec,
    local_sems,
    hello,
    x_recv,
    d_recv,
    f_recv,
    p_recv,
    r_recv,
):
    ep = lax.axis_index("ep")
    tp = lax.axis_index("tp")
    other = 1 - tp
    z = lax.div(ep, 16)
    y = lax.rem(lax.div(ep, 4), 4)
    x = lax.rem(ep, 4)
    z_at = [lax.rem(z + d, 4) * 16 for d in range(4)]
    y_at = [lax.rem(y + d, 4) * 4 for d in range(4)]
    x_at = [lax.rem(x + d, 4) for d in range(4)]

    def peer_of(p, sign):
        dz, dy, dx = STEPS[p]
        return z_at[sign * dz % 4] + y_at[sign * dy % 4] + x_at[sign * dx % 4]

    pairs = (
        (x_in, xv.at[tp], 0),
        (in_proj_in, in_proj, 5),
        (decay_in, rates.at[0], 1),
        (freq_in, rates.at[1], 1),
        (step_in, step, 2),
        (imap_in, maps.at[0], 3),
        (omap_in, maps.at[1], 3),
        (mix_gain_in, mix_gain, 6),
        (state_in, state, 4),
        (pscale_in, pscale, 7),
        (ids_in, ids, 8),
        (wts_in, wts, 9),
        (out_gain_in, out_gain, 10),
        (ffn_gain_in, ffn_gain, 12),
        (out_proj_in, out_proj, 11),
        (wg_in, wgu.at[0], 0),
        (wu_in, wgu.at[1], 0),
        (wd_in, wd, 1),
    )

    def loaded(ref, sem):
        pltpu.make_async_copy(ref, ref, local_sems.at[sem]).wait()

    loads = [pltpu.make_async_copy(a, b, local_sems.at[i]) for a, b, i in pairs]
    loads[0].start()
    barrier = pltpu.get_barrier_semaphore()

    @pl.when(tp == 0)
    def _():
        pl.semaphore_signal(barrier, inc=1, device_id=(ep, other), device_id_type=MESH)

    for load in loads[1:14]:
        load.start()

    @pl.when(tp == 1)
    def _():
        pl.semaphore_wait(barrier, 1)
        pl.semaphore_signal(hello, inc=1, device_id=(ep, other), device_id_type=MESH)

    @pl.when(tp == 0)
    def _():
        pl.semaphore_wait(hello, 1)

        def greet(i, carry):
            pl.semaphore_signal(
                barrier, inc=1, device_id=(lax.rem(ep + i, PEERS), tp), device_id_type=MESH
            )
            return carry

        lax.fori_loop(1, PEERS, greet, 0)


    loaded(xv.at[tp], 0)

    def to_partner(ref, send, recv_):
        return pltpu.make_async_remote_copy(
            src_ref=ref, dst_ref=ref, send_sem=send, recv_sem=recv_,
            device_id=(ep, other), device_id_type=MESH,
        )

    x_copy = to_partner(xv.at[tp], local_sems.at[0], x_recv.at[2])
    x_copy.start()

    loaded(rates, 1)
    loaded(step, 2)
    rate_real = -rates[0]
    rate_imag = rates[1]
    n_groups, n_state = rate_real.shape
    diag = iota((n_groups, n_groups), 0) == iota((n_groups, n_groups), 1)
    time_step = jnp.sum(jnp.where(diag, step[...], 0.0), axis=1, keepdims=True)
    magnitude = jnp.exp(rate_real * time_step)
    phase = rate_imag * time_step
    bar_real = magnitude * jnp.cos(phase)
    bar_imag = magnitude * jnp.sin(phase)
    denominator = rate_real * rate_real + rate_imag * rate_imag
    shifted = bar_real - 1.0
    coef_real = (shifted * rate_real + bar_imag * rate_imag) / denominator
    coef_imag = (bar_imag * rate_real - shifted * rate_imag) / denominator
    own_group = iota((n_groups, STATES), 0) == (iota((n_groups, STATES), 1) >> 6)

    def as_row(v):
        wide = jnp.concatenate([v] * (STATES // n_state), axis=1)
        return jnp.sum(jnp.where(own_group, wide, 0.0), axis=0, keepdims=True)

    bar_real, bar_imag, coef_real, coef_imag = (
        as_row(v) for v in (bar_real, bar_imag, coef_real, coef_imag)
    )

    same = (iota((128, 512), 0) >> 4) == (iota((128, 512), 1) >> 6)

    def spread_groups(m):
        return jnp.where(same, jnp.concatenate([m] * 8, axis=1), 0.0).astype(BF16)

    loaded(maps, 3)
    for b in range(4):
        rows = slice(b * 128, (b + 1) * 128)
        for i in range(2):
            inmix[i, rows, :] = spread_groups(maps[0, i, rows, :])
        outmix[0, rows, :] = spread_groups(maps[1, 0, rows, :])
        outmix[1, rows, :] = spread_groups(-maps[1, 1, rows, :])

    loaded(state, 4)
    for b in range(4):
        cols = slice(b * 512, (b + 1) * 512)
        hr = state[0, :, cols]
        hi = state[1, :, cols]
        br, bi = bar_real[:, cols], bar_imag[:, cols]
        nstate[0, :, cols] = br * hr - bi * hi
        nstate[1, :, cols] = br * hi + bi * hr
    loaded(in_proj, 5)
    loaded(mix_gain, 6)
    loaded(pscale, 7)
    x_copy.wait()
    x0 = xv[0].astype(F32)
    x1 = xv[1].astype(F32)
    mean_sq = (
        jnp.sum(x0 * x0, axis=1, keepdims=True) + jnp.sum(x1 * x1, axis=1, keepdims=True)
    ) * (1.0 / (2 * HALF))
    scale = lax.rsqrt(mean_sq + EPS)
    n0 = (x0 * scale * mix_gain[:, :HALF]).astype(BF16)
    n1 = (x1 * scale * mix_gain[:, HALF:]).astype(BF16)
    for load in loads[14:]:
        load.start()
    channels = (mm(n0, in_proj[:HALF, :]) + mm(n1, in_proj[HALF:, :])).astype(BF16)
    spans = [(slice(b * 128, (b + 1) * 128), slice(b * 512, (b + 1) * 512)) for b in range(4)]
    pushes = [
        (mm(channels[:, rows], inmix[0, rows, :]), mm(channels[:, rows], inmix[1, rows, :]))
        for rows, _ in spans
    ]
    states = []
    for (rows, cols), (u0, u1) in zip(spans, pushes):
        cr, ci = coef_real[:, cols], coef_imag[:, cols]
        nr = nstate[0, :, cols] + (cr * u0 - ci * u1)
        ni = nstate[1, :, cols] + (cr * u1 + ci * u0)
        nstate[0, :, cols] = nr
        nstate[1, :, cols] = ni
        states.append((nr.astype(BF16), ni.astype(BF16)))
    mixed = jnp.concatenate(
        [
            mm_nt(nr, outmix[0, rows, :]) + mm_nt(ni, outmix[1, rows, :])
            for (rows, _), (nr, ni) in zip(spans, states)
        ],
        axis=1,
    ) + pscale[...] * channels.astype(F32)
    actx[tp] = jax.nn.gelu(mixed, approximate=True).astype(BF16)

    store_state = pltpu.make_async_copy(nstate, nstate_ref, local_sems.at[5])
    store_state.start()
    act_copy = to_partner(actx.at[tp], local_sems.at[3], x_recv.at[0])
    act_copy.start()

    loaded(ids, 8)
    loaded(wts, 9)
    expert = iota((PEERS, SEQ), 0)
    named = jnp.zeros((PEERS, SEQ), F32)
    weight = jnp.zeros((PEERS, SEQ), F32)
    for k in range(4):
        hit = ids[k : k + 1, :] == expert
        named = named + jnp.where(hit, 1.0, 0.0)
        weight = weight + jnp.where(hit, wts[k : k + 1, :], 0.0)
    earlier = jnp.where(iota((SEQ, SEQ), 0) < iota((SEQ, SEQ), 1), 1.0, 0.0).astype(BF16)
    slot_of = named * (mm(named.astype(BF16), earlier) + 1.0)
    pos = iota((PEERS, PEERS), 0)
    named_at = jnp.zeros((PEERS, PEERS), jnp.int32)
    for p in range(PEERS):
        named_at = jnp.where(pos == p, peer_of(p, 1), named_at)
    order = jnp.where(named_at == iota((PEERS, PEERS), 1), 1.0, 0.0).astype(BF16)
    w_hi = weight.astype(BF16)
    slot_pt = mm(order, slot_of.astype(BF16)).astype(BF16)
    eye = jnp.where(iota((SEQ, SEQ), 0) == iota((SEQ, SEQ), 1), 1.0, 0.0).astype(BF16)

    def turned(v):
        return mm_nt(eye, v).astype(BF16)

    slot_tp = turned(slot_pt)
    whi_tp = turned(mm(order, w_hi).astype(BF16))

    slot_p4 = jnp.concatenate([slot_pt] * QUARTERS, axis=1)
    row = iota((GROWS, QUARTERS * SEQ), 0)
    rowp = div_small(row, ROWS)
    rem_row = row - rowp * ROWS
    rowq = div_small(rem_row, SLOTS)
    rows_ = rem_row - rowq * SLOTS
    want = jnp.where(rowq == (iota((GROWS, QUARTERS * SEQ), 1) >> 6), rows_ + 1, -1).astype(F32)
    spread_row = div_small(iota((GROWS, PEERS), 0), ROWS)
    spread_col = iota((GROWS, PEERS), 1)
    for b in range(GROUPS):
        spread = jnp.where(spread_row + b * 8 == spread_col, 1.0, 0.0).astype(BF16)
        onehot[b * GROWS : (b + 1) * GROWS, :] = jnp.where(
            mm(spread, slot_p4) == want, 1.0, 0.0
        ).astype(BF16)

    loaded(out_gain, 10)
    loaded(out_proj, 11)
    loaded(ffn_gain, 12)
    act_copy.wait()
    a0 = actx[0].astype(F32)
    a1 = actx[1].astype(F32)
    mean_sq = (
        jnp.sum(a0 * a0, axis=1, keepdims=True) + jnp.sum(a1 * a1, axis=1, keepdims=True)
    ) * (1.0 / (2 * CHAN))
    scale = lax.rsqrt(mean_sq + EPS)
    s0 = (a0 * scale * out_gain[:, :CHAN]).astype(BF16)
    s1 = (a1 * scale * out_gain[:, CHAN:]).astype(BF16)
    after = (
        xv[tp].astype(F32) + (mm(s0, out_proj[:CHAN, :]) + mm(s1, out_proj[CHAN:, :]))
    ).astype(BF16)
    outv[...] = after
    after32 = after.astype(F32)
    sqx[tp] = jnp.broadcast_to(jnp.sum(after32 * after32, axis=1, keepdims=True), (SEQ, 128))
    sq_copy = to_partner(sqx.at[tp], local_sems.at[4], x_recv.at[1])
    sq_copy.start()

    @pl.when(tp == 0)
    def _():
        pl.semaphore_wait(barrier, PEERS - 1)
        pl.semaphore_signal(hello, inc=1, device_id=(ep, other), device_id_type=MESH)

    def send_block(src, dst, p, sign, send, recv_):
        at = pl.ds(p * ROWS, ROWS)
        pltpu.make_async_remote_copy(
            src_ref=src.at[at], dst_ref=dst.at[at], send_sem=send, recv_sem=recv_,
            device_id=(peer_of(p, sign), tp), device_id_type=MESH,
        ).start()

    def gather(b, values):
        stacked = jnp.concatenate(
            [values[:, q * QW : (q + 1) * QW] for q in range(QUARTERS)], axis=0
        )
        rows = slice(b[0] * GROWS, (b[-1] + 1) * GROWS)
        sendbuf[rows, :] = mm(onehot[rows, :], stacked).astype(BF16)

    def dispatch(b):
        for p in range(b[0] * GP, min((b[-1] + 1) * GP, PEERS - 1)):
            send_block(sendbuf, recv.at[tp], p, 1, local_sems.at[7], d_recv.at[UNIT_OF[p // GP]])


    gather(CHUNKS[0], after)

    @pl.when(tp == 1)
    def _():
        pl.semaphore_wait(hello, 1)

    dispatch(CHUNKS[0])

    def block_perm(rdim, cdim):
        r = iota((GROWS, GROWS), rdim)
        c = iota((GROWS, GROWS), cdim)
        rq = div_small(r, GSLOTS)
        rr = r - rq * GSLOTS
        rp = div_small(rr, SLOTS)
        rs = rr - rp * SLOTS
        return jnp.where(rp * ROWS + rq * SLOTS + rs == c, 1.0, 0.0).astype(BF16)

    perm[...] = block_perm(0, 1)
    permt[...] = block_perm(1, 0)

    sq_copy.wait()
    mean_sq = (sqx[0] + sqx[1])[:, :1] * (1.0 / (2 * HALF))
    expert_in = (after32 * lax.rsqrt(mean_sq + EPS) * ffn_gain[tp]).astype(BF16)
    for b in CHUNKS[1:]:
        gather(b, expert_in)
        dispatch(b)
    recv[tp, OWN:ALL, :] = sendbuf[OWN:ALL, :]

    col = iota((PEERS, ALL), 1)
    spread_t = jnp.where(div_small(col, ROWS) == iota((PEERS, ALL), 0), 1.0, 0.0).astype(BF16)
    c1 = iota((1, ALL), 1)
    c1 = c1 - div_small(c1, ROWS) * ROWS
    cq = div_small(c1, SLOTS)
    cs = (c1 - cq * SLOTS + 1).astype(F32)
    slot_x = mm(slot_tp, spread_t)
    whi_x = mm(whi_tp, spread_t)
    hit = slot_x == cs
    for q in range(QUARTERS):
        keep = hit & (cq == q)
        chi[q * SEQ : (q + 1) * SEQ, :] = jnp.where(keep, whi_x, 0.0).astype(BF16)

    loaded(wgu, 0)
    loaded(wd, 1)

    def arrived(ref, sem):
        pltpu.make_async_remote_copy(
            src_ref=ref, dst_ref=ref, send_sem=sem, recv_sem=sem,
            device_id=(ep, other), device_id_type=MESH,
        ).wait_recv()

    def passed_on(u):
        first = UNITS[u][0] * GROWS
        last = (UNITS[u][-1] + 1) * GROWS
        return first, last, to_partner(
            recv.at[tp, pl.ds(first, last - first)], local_sems.at[9], f_recv.at[u]
        )

    def forward(u):
        first, last, copy = passed_on(u)
        arrived(recv.at[tp, pl.ds(first, min(last, OWN) - first)], d_recv.at[u])
        copy.start()

    def assemble(g):
        slots = slice(g * GSLOTS, (g + 1) * GSLOTS)
        moved = [mm(perm[...], recv[h, g * GROWS : (g + 1) * GROWS, :]) for h in range(2)]
        pieces = [
            (h, slice(q * QW, (q + 1) * QW), moved[h][q * GSLOTS : (q + 1) * GSLOTS, :])
            for h in range(2)
            for q in range(QUARTERS)
        ]
        if g in CHUNKS[0]:
            squares = pieces[0][2] * pieces[0][2]
            for _, _, piece in pieces[1:]:
                squares = squares + piece * piece
            mean_sq = jnp.sum(squares, axis=1, keepdims=True) * (1.0 / (2 * HALF))
            scale = lax.rsqrt(mean_sq + EPS)
            pieces = [(h, at, piece * scale * ffn_gain[h, :, at]) for h, at, piece in pieces]
        for h, at, piece in pieces:
            amat[slots, h * HALF + at.start : h * HALF + at.stop] = piece.astype(BF16)

    def experts(order):
        units_of = [[u for u in range(len(UNITS)) if UNITS[u][0] in CHUNKS[c]] for c in order] + [[]]
        for u in units_of[0]:
            forward(u)
        for u in units_of[0]:
            passed_on(u)[2].wait_recv()
            for g in UNITS[u]:
                assemble(g)

        def units(c, halves):
            srows = slice(CHUNKS[c][0] * GSLOTS, (CHUNKS[c][-1] + 1) * GSLOTS)
            lhs = amat[srows, :]
            for n in halves:
                at = slice(n * 512, (n + 1) * 512)
                gate = mm(lhs, wgu[0, :, at])
                up = mm(lhs, wgu[1, :, at])
                gated = jnp.minimum(gate, LIMIT)
                act = (jnp.clip(up, -LIMIT, LIMIT) + 1.0) * gated * jax.nn.sigmoid(ALPHA * gated)
                hid[srows, at] = act.astype(BF16)

        for i, c in enumerate(order):
            chunk = CHUNKS[c]
            last = i + 1 == len(order)
            srows = slice(chunk[0] * GSLOTS, (chunk[-1] + 1) * GSLOTS)
            if i == 1:
                for u in units_of[i + 1]:
                    forward(u)
            units(c, (1,) if i >= AHEAD else (0, 1))
            if i == 0:
                for u in units_of[i + 1]:
                    forward(u)
            lhs = hid[srows, :]
            pieces = 2 if last else 1
            width = HALF // pieces
            parts = []
            for n in range(pieces):
                at = pl.ds(n * width, width)
                wat = pl.ds(pl.multiple_of(other * HALF + n * width, 512), width)
                psend[srows, at] = mm(lhs, wd[:, wat]).astype(BF16)
                part_copy = pltpu.make_async_remote_copy(
                    src_ref=psend.at[srows, at], dst_ref=prec.at[srows, at],
                    send_sem=local_sems.at[10], recv_sem=p_recv.at[i + n],
                    device_id=(ep, other), device_id_type=MESH,
                )
                part_copy.start()
                parts.append(part_copy)
            if i == 1:
                for u in units_of[i + 1]:
                    passed_on(u)[2].wait_recv()
            own[srows, :] = mm(lhs, wd[:, pl.ds(pl.multiple_of(tp * HALF, HALF), HALF)]).astype(BF16)
            if i > 0:
                for u in units_of[i + 1]:
                    for g in UNITS[u]:
                        assemble(g)
            if not last and i + 1 >= AHEAD:
                units(order[i + 1], (0,))
            for part_copy in parts:
                part_copy.wait_recv()
            for g in chunk:
                slots = slice(g * GSLOTS, (g + 1) * GSLOTS)
                both = (own[slots, :].astype(F32) + prec[slots, :].astype(F32)).astype(BF16)
                tall = jnp.concatenate(
                    [both[:, q * QW : (q + 1) * QW] for q in range(QUARTERS)], axis=0
                )
                rsend[g * GROWS : (g + 1) * GROWS, :] = mm(permt[...], tall).astype(BF16)
            for g in chunk:
                for p in range(g * GP, min((g + 1) * GP, PEERS - 1)):
                    send_block(rsend, rrecv, p, -1, local_sems.at[8], r_recv.at[c])
            if i == 0:
                for u in units_of[1]:
                    passed_on(u)[2].wait_recv()
                for u in units_of[1]:
                    for g in UNITS[u]:
                        assemble(g)

    experts(tuple(range(len(CHUNKS))))
    rrecv[OWN:ALL, :] = rsend[OWN:ALL, :]

    total = jnp.zeros((QUARTERS * SEQ, QW), F32)
    for c, chunk in enumerate(CHUNKS):
        first = chunk[0] * GROWS
        last = (chunk[-1] + 1) * GROWS
        arrived(rrecv.at[pl.ds(first, min(last, OWN) - first)], r_recv.at[c])
        got = rrecv[first:last, :]
        total = total + mm(chi[:, first:last], got)
    for q in range(QUARTERS):
        cols = slice(q * QW, (q + 1) * QW)
        outv[:, cols] = (
            outv[:, cols].astype(F32) + total[q * SEQ : (q + 1) * SEQ, :]
        ).astype(BF16)
    store_out = pltpu.make_async_copy(outv, out_ref, local_sems.at[6])
    store_out.start()
    for sem, sent in (
        (7, sendbuf.at[pl.ds(0, OWN)]),
        (8, rsend.at[pl.ds(0, OWN)]),
        (9, recv.at[tp, pl.ds(0, ALL)]),
        (10, psend),
    ):
        pltpu.make_async_remote_copy(
            src_ref=sent, dst_ref=sent, send_sem=local_sems.at[sem], recv_sem=local_sems.at[sem],
            device_id=(ep, other), device_id_type=MESH,
        ).wait_send()
    store_state.wait()
    store_out.wait()


def store(u_in, s_in, u_out, s_out, u_buf, s_buf, in_sems, out_sems):
    pieces = [
        (s_in.at[i, pl.ds(r, 32)], s_buf.at[i, pl.ds(r, 32)], s_out.at[i, pl.ds(r, 32)])
        for i in range(2)
        for r in range(0, SEQ, 32)
    ]
    pieces.append((u_in, u_buf, u_out))
    loads = [pltpu.make_async_copy(a, b, in_sems.at[i]) for i, (a, b, _) in enumerate(pieces)]
    stores = [pltpu.make_async_copy(b, c, out_sems.at[i]) for i, (_, b, c) in enumerate(pieces)]
    for load in loads:
        load.start()
    for load, put in zip(loads, stores):
        load.wait()
        put.start()
    for put in stores:
        put.wait()


def local(
    residual,
    route_ids,
    route_weights,
    carried_state,
    mix_gain,
    in_proj,
    decay_rate,
    frequency,
    step_size,
    input_map,
    output_matrix,
    passthrough_scale,
    out_gain,
    out_proj,
    ffn_gain,
    w_gate,
    w_up,
    w_down,
):
    ids, wts = route_ids.T, route_weights.T
    maps = (
        jnp.swapaxes(input_map, 2, 3).reshape(2, CHAN, -1),
        output_matrix.reshape(2, CHAN, -1),
    )
    args = (
        residual,
        ids,
        wts,
        decay_rate,
        frequency,
        step_size.reshape(1, -1),
        *maps,
        mix_gain.reshape(1, -1),
        in_proj,
        carried_state,
        passthrough_scale.reshape(1, -1),
        out_gain.reshape(1, -1),
        out_proj,
        ffn_gain.reshape(2, 1, -1),
        w_gate.reshape(w_gate.shape[1:]),
        w_up.reshape(w_up.shape[1:]),
        w_down.reshape(w_down.shape[1:]),
    )
    dma = pltpu.SemaphoreType.DMA
    vmem = pltpu.VMEM
    out_shape = (
        jax.ShapeDtypeStruct(residual.shape, BF16),
        jax.ShapeDtypeStruct(carried_state.shape, F32),
    )
    results = pl.pallas_call(
        kernel,
        out_shape=out_shape,
        in_specs=[pl.BlockSpec(memory_space=pl.ANY)] * len(args),
        out_specs=(pl.BlockSpec(memory_space=pl.ANY),) * 2,
        scratch_shapes=[
            vmem(residual.shape, BF16),
            vmem(carried_state.shape, F32),
            vmem((2, *residual.shape), BF16),
        ]
        + [vmem(a.shape, a.dtype) for a in (ids, wts)]
        + [
            vmem((2, *decay_rate.shape), F32),
            vmem((1, step_size.shape[0]), F32),
            vmem((2, *maps[0].shape), F32),
            vmem((1, mix_gain.shape[0]), F32),
            vmem(in_proj.shape, BF16),
            vmem(carried_state.shape, F32),
            vmem((1, CHAN), F32),
            vmem((1, 2 * CHAN), F32),
            vmem(out_proj.shape, BF16),
            vmem((2, 1, HALF), F32),
            vmem((2, *w_gate.shape[1:]), BF16),
            vmem(w_down.shape[1:], BF16),
            vmem((2, CHAN, 512), BF16),
            vmem((2, CHAN, 512), BF16),
            vmem((2, SEQ, CHAN), BF16),
            vmem((2, SEQ, 128), F32),
            vmem((ALL, QUARTERS * SEQ), BF16),
            vmem((QUARTERS * SEQ, ALL), BF16),
            vmem((GROWS, GROWS), BF16),
            vmem((GROWS, GROWS), BF16),
            vmem((PAD, QW), BF16),
            vmem((2, PAD, QW), BF16),
            vmem((PAD, QW), BF16),
            vmem((PAD, QW), BF16),
            vmem((PEERS * SLOTS, 2 * HALF), BF16),
            vmem((PEERS * SLOTS, HALF), BF16),
            vmem((PEERS * SLOTS, HALF), BF16),
            vmem((PEERS * SLOTS, HALF), BF16),
            vmem((PEERS * SLOTS, HALF), BF16),
            dma((13,)),
            pltpu.SemaphoreType.REGULAR,
            dma((3,)),
            dma((len(UNITS),)),
            dma((len(UNITS),)),
            dma((len(CHUNKS) + 1,)),
            dma((len(CHUNKS),)),
        ],
        compiler_params=pltpu.CompilerParams(
            collective_id=0, has_side_effects=True, vmem_limit_bytes=VMEM_LIMIT
        ),
    )(*args)
    return pl.pallas_call(
        store,
        out_shape=out_shape,
        in_specs=[pl.BlockSpec(memory_space=pl.ANY)] * 2,
        out_specs=(pl.BlockSpec(memory_space=pl.ANY),) * 2,
        scratch_shapes=[
            vmem(residual.shape, BF16),
            vmem(carried_state.shape, F32),
            dma((5,)),
            dma((5,)),
        ],
        compiler_params=pltpu.CompilerParams(vmem_limit_bytes=VMEM_LIMIT),
    )(*results)


def solution(mesh):
    placed = (
        P("ep", "tp"),
        P("ep", None),
        P("ep", None),
        P(None, "ep", "tp"),
        P(),
        P(None, "tp"),
        P("tp", None),
        P("tp", None),
        P("tp"),
        P(None, "tp", None, None),
        P(None, "tp", None, None),
        P("tp"),
        P(),
        P(None, "tp"),
        P(),
        P("ep", None, "tp"),
        P("ep", None, "tp"),
        P("ep", "tp", None),
    )
    return jax.shard_map(
        local,
        mesh=mesh,
        in_specs=placed,
        out_specs=(P("ep", "tp"), P(None, "ep", "tp")),
        check_vma=False,
    )
```
